512 devices in a mesh: grp: 2 (over y), sp: 64 (over z, core), tp: 4 (over x).
Axes of the slice: x: 4, y: 2, z: 32, core: 2. Of those that a mesh axis runs over, the one named last changes fastest.
The devices are a block of a 4x8x32 slice.
Arguments:
- query_latent: bfloat16 [16384, 768], P(('grp', 'sp')), parts along dimension 0, may hold values from -6 to 6
- key_latent: bfloat16 [16384, 256], P(('grp', 'sp', 'tp')), parts along dimension 0, may hold values from -20 to 20
- rotary_key: bfloat16 [16384, 64], P(('grp', 'sp', 'tp')), parts along dimension 0, may hold values from -1000 to 1000
- query_gain: float32 [768], replicated, may hold values from 0.1 to 1.9
- latent_gain: float32 [256], replicated, may hold values from 0.1 to 1.9
- query_up: bfloat16 [768, 3072], P(None, 'tp'), may hold values from -0.21875 to 0.21875
- key_up: bfloat16 [256, 2048], P(None, 'tp'), may hold values from -0.375 to 0.375
- value_up: bfloat16 [256, 2048], P(None, 'tp'), may hold values from -0.375 to 0.375
- out_gain: float32 [2048], P('tp'), may hold values from 0.1 to 1.9
- out_weight: bfloat16 [2048, 4096], P('sp', 'tp'), may hold values from -0.125 to 0.125
Outputs:
- mixed: bfloat16 [16384, 4096], P(('grp', 'sp'), 'tp'), parts along dimension 0
The draws below stay inside these ranges and needn't reach their ends.
There are 2 independent parts, one for each index of `grp`. The reference program is written for one: setup_inputs(seed, part) draws one part's arguments, and reference() takes and returns one part's arrays. A program takes and returns all parts, laid end to end along the dimension named above; an argument that names none is the same for every part. Nothing has to cross between parts.
All inputs are finite; a program needn't handle non-finite values.
Results may differ from the reference program's by a relative error of at most 0.02.
The reference program's roundings to bfloat16 on the way count: a program that leaves them out, or rounds other values in their place, can miss the bound.
Values may be sent and summed in bfloat16 or wider, within the bound.
No kernel may reach another device: no remote copies, remote signals or barrier semaphores. Data moves between devices by JAX's collectives and lax.ppermute only.
A program may use at most 128 MiB of HBM per device.

```python
import jax
import jax.numpy as jnp
from jax import lax

D_MODEL = 4096
HEADS = 16
NOPE_DIM = 128
ROPE_DIM = 64
VALUE_DIM = 128
QRANK = 768
KVRANK = 256
TOK_DEV = 128
TOKENS = 8192
N_SP = 64


def draw_key_latent(key, part):
    first_key, second_key = jax.random.split(jax.random.fold_in(key, 11), 2)
    blocks = TOKENS // TOK_DEV
    offsets = jax.random.normal(second_key, (blocks, KVRANK), jnp.float32)
    noise = jax.random.normal(first_key, (TOKENS, KVRANK), jnp.float32)
    offset_rows = jnp.repeat(offsets, TOK_DEV, axis=0)
    return jnp.clip(noise + offset_rows, -20.0, 20.0).astype(jnp.bfloat16)


def draw_rotary_key(key, part):
    first_key = jax.random.fold_in(jax.random.fold_in(key, 23), 0)
    values = jax.random.normal(first_key, (TOKENS, ROPE_DIM), jnp.float32)
    return jnp.clip(values, -1000.0, 1000.0).astype(jnp.bfloat16)


def shard_levels(rng, extent, cuts, smallest, top_value):
    def one(dim, shards_of):
        heights = jax.random.uniform(jax.random.fold_in(jax.random.fold_in(rng, 6), dim), (shards_of,), jnp.float32, smallest / len(cuts), top_value / len(cuts))
        return jnp.repeat(jnp.exp(heights), extent[dim] // shards_of).reshape((-1,) + (1,) * (len(extent) - dim - 1))

    factor_of = one(*cuts[0])
    for cut in cuts[1:]:
        factor_of = factor_of * one(*cut)
    return factor_of


def scatter_about(own_key, extent, scale, reach, pieces=(), kind=jnp.bfloat16):
    result = jax.random.normal(own_key, extent, jnp.float32) * scale
    if len(pieces) > 0:
        result = shard_levels(own_key, extent, pieces, -0.22, 0.18) * result
    return jnp.clip(result, min=-reach, max=reach).astype(kind)


def setup_inputs(seed: int = 0, part: int = 0) -> dict:
    keys = jax.random.split(jax.random.key(seed), 11)
    own_keys = jax.random.split(jax.random.fold_in(keys[10], part), 11)
    return {
        "query_latent": scatter_about(own_keys[0], (TOKENS, QRANK), 1.0, 6.0, ((0, 64),)),
        "key_latent": draw_key_latent(jax.random.fold_in(jax.random.fold_in(keys[10], part), 71), part),
        "rotary_key": draw_rotary_key(jax.random.fold_in(jax.random.fold_in(keys[10], part), 71), part),
        "query_gain": jnp.clip(1.0 + 0.18 * jax.random.normal(keys[3], (QRANK,), jnp.float32), 0.1, 1.9),
        "latent_gain": jnp.clip(1.0 + 0.18 * jax.random.normal(keys[4], (KVRANK,), jnp.float32), 0.1, 1.9),
        "query_up": scatter_about(keys[5], (QRANK, HEADS * (NOPE_DIM + ROPE_DIM)), QRANK ** -0.5, 0.21875, ((1, 4),)),
        "key_up": scatter_about(keys[6], (KVRANK, HEADS * NOPE_DIM), KVRANK ** -0.5, 0.375, ((1, 4),)),
        "value_up": scatter_about(keys[7], (KVRANK, HEADS * VALUE_DIM), KVRANK ** -0.5, 0.375, ((1, 4),)),
        "out_gain": jnp.clip(1.0 + 0.18 * jax.random.normal(keys[8], (HEADS * VALUE_DIM,), jnp.float32), 0.1, 1.9),
        "out_weight": scatter_about(keys[9], (HEADS * VALUE_DIM, D_MODEL), (HEADS * VALUE_DIM) ** -0.5, 0.125, ((0, 64), (1, 4))),
    }


norm_eps = 1e-06
rope_theta = 10000.0

def rms_scaled(inputs, gain_vec):
    widened = inputs.astype(jnp.float32)
    return widened * lax.rsqrt(lax.optimization_barrier(jnp.mean(widened * widened, axis=-1, keepdims=True)) + norm_eps) * gain_vec

def rotate_half(inputs, positions):
    half_width = inputs.shape[-1] // 2
    inverse = rope_theta ** (-jnp.arange(half_width, dtype=jnp.float32) / half_width)
    angles = positions[:, None] * inverse[None, :]
    if inputs.ndim == 3:
        angles = angles[:, None, :]
    cosine = jnp.cos(angles)
    sine = jnp.sin(angles)
    widened = inputs.astype(jnp.float32)
    first = widened[..., :half_width]
    second = widened[..., half_width:]
    return jnp.concatenate([first * cosine - second * sine, second * cosine + first * sine], axis=-1)

def reference(query_latent, key_latent, rotary_key, query_gain, latent_gain, query_up, key_up, value_up, out_gain, out_weight):
    positions = jnp.arange(TOKENS, dtype=jnp.float32)
    score_scale = (NOPE_DIM + ROPE_DIM) ** (-0.5)
    query_normed = rms_scaled(query_latent, query_gain).astype(jnp.bfloat16)
    query_full = jnp.dot(query_normed, query_up, preferred_element_type=jnp.float32).astype(jnp.bfloat16)
    query_full = query_full.reshape(TOKENS, HEADS, NOPE_DIM + ROPE_DIM)
    query_plain = query_full[..., :NOPE_DIM]
    query_turned = rotate_half(query_full[..., NOPE_DIM:], positions).astype(jnp.bfloat16)
    latent_normed = rms_scaled(key_latent, latent_gain).astype(jnp.bfloat16)
    key_turned = rotate_half(rotary_key, positions).astype(jnp.bfloat16)
    key_plain = jnp.dot(latent_normed, key_up, preferred_element_type=jnp.float32).astype(jnp.bfloat16)
    key_wide = key_plain.reshape(TOKENS, HEADS, NOPE_DIM).astype(jnp.float32)
    turned_wide = key_turned.astype(jnp.float32)
    latent_wide = latent_normed.astype(jnp.float32)
    value_heads = value_up.astype(jnp.float32).reshape(KVRANK, HEADS, VALUE_DIM)

    def one_block(block_index):
        begin = (block_index * TOK_DEV).astype(jnp.int32)
        plain = lax.dynamic_slice_in_dim(query_plain, begin, TOK_DEV, 0).astype(jnp.float32)
        turned = lax.dynamic_slice_in_dim(query_turned, begin, TOK_DEV, 0).astype(jnp.float32)
        scores = jnp.einsum('qhd,khd->qhk', plain, key_wide) + jnp.einsum('qhd,kd->qhk', turned, turned_wide)
        scores = scores * score_scale
        row_top = lax.optimization_barrier(jnp.max(scores, axis=-1, keepdims=True))
        expo = jnp.exp(scores - row_top)
        total = lax.optimization_barrier(jnp.sum(expo, axis=-1))
        weights = lax.optimization_barrier(expo.astype(jnp.bfloat16)).astype(jnp.float32)
        latent_mix = jnp.einsum('qhk,kc->qhc', weights, latent_wide) / total[..., None]
        latent_mix = lax.optimization_barrier(latent_mix.astype(jnp.bfloat16)).astype(jnp.float32)
        head_out = jnp.einsum('qhc,chd->qhd', latent_mix, value_heads).astype(jnp.bfloat16)
        return head_out.reshape(TOK_DEV, HEADS * VALUE_DIM)
    head_out = lax.map(one_block, jnp.arange(N_SP, dtype=jnp.int32)).reshape(TOKENS, HEADS * VALUE_DIM)
    widened = head_out.astype(jnp.float32)
    mean_square = lax.optimization_barrier(jnp.mean(widened * widened, axis=1))
    gained = (widened * out_gain).astype(jnp.bfloat16)
    projected = jnp.dot(gained, out_weight, preferred_element_type=jnp.float32)
    return (projected * lax.rsqrt(mean_square + norm_eps)[:, None]).astype(jnp.bfloat16)
```

```python
import functools

import jax
import jax.numpy as jnp
from jax import lax
from jax.experimental import pallas as pl
from jax.experimental.pallas import tpu as pltpu
from jax.sharding import Mesh
from jax.sharding import PartitionSpec as P

HEADS = 16
NOPE_DIM = 128
ROPE_DIM = 64
VALUE_DIM = 128
KVRANK = 256
CORES = 2


norm_eps = 1e-06
rope_theta = 10000.0
score_scale = (NOPE_DIM + ROPE_DIM) ** (-0.5)
exp2_scale = score_scale * 1.4426950408889634


def rms_scaled(inputs, gain_vec):
    widened = inputs.astype(jnp.float32)
    return (
        widened
        * lax.rsqrt(jnp.mean(widened * widened, axis=-1, keepdims=True) + norm_eps)
        * gain_vec
    )


def rotate_half(inputs, positions):
    half_width = inputs.shape[-1] // 2
    inverse = rope_theta ** (-jnp.arange(half_width, dtype=jnp.float32) / half_width)
    angles = positions[:, None] * inverse[None, :]
    if inputs.ndim == 3:
        angles = angles[:, None, :]
    cosine = jnp.cos(angles)
    sine = jnp.sin(angles)
    widened = inputs.astype(jnp.float32)
    first = widened[..., :half_width]
    second = widened[..., half_width:]
    return jnp.concatenate(
        [first * cosine - second * sine, second * cosine + first * sine], axis=-1
    )


def attend_kernel(n_keys, first, row_tile, q_ref, *refs):
    key_refs = refs[:n_keys]
    refs = refs[n_keys:]
    if first:
        top_out, sum_out, mix_out = refs
    else:
        top_in, sum_in, mix_in, top_out, sum_out, mix_out = refs
    rows = q_ref.shape[0]
    for begin in range(0, rows, row_tile):
        span = pl.ds(begin, row_tile)
        q = q_ref[span, :]
        if first:
            top = total = mix = None
        else:
            top = top_in[span, :1]
            total = sum_in[span, :1]
            mix = mix_in[span, :]
        for key_ref in key_refs:
            keys = key_ref[...]
            scores = lax.dot_general(
                q, keys, (((1,), (1,)), ((), ())), preferred_element_type=jnp.float32
            )
            here = jnp.max(scores, axis=1, keepdims=True)
            new_top = here if top is None else jnp.maximum(top, here)
            expo = jnp.exp2((scores - new_top) * exp2_scale)
            part = jnp.sum(expo, axis=1, keepdims=True)
            moved = jnp.dot(
                expo.astype(jnp.bfloat16),
                keys[:, :KVRANK],
                preferred_element_type=jnp.float32,
            )
            if top is None:
                total, mix = part, moved
            else:
                rescale = jnp.exp2((top - new_top) * exp2_scale)
                total = total * rescale + part
                mix = mix * rescale + moved
            top = new_top
        top_out[span, :] = jnp.broadcast_to(top, (row_tile, 128))
        sum_out[span, :] = jnp.broadcast_to(total, (row_tile, 128))
        mix_out[span, :] = mix


def attend(queries, key_parts, state, row_tile=256):
    rows, width = queries.shape
    keys = sum(k.shape[0] for k in key_parts)
    first = state is None
    state = () if first else state
    shapes = (
        jax.ShapeDtypeStruct((rows, 128), jnp.float32),
        jax.ShapeDtypeStruct((rows, 128), jnp.float32),
        jax.ShapeDtypeStruct((rows, KVRANK), jnp.float32),
    )
    return pl.pallas_call(
        functools.partial(attend_kernel, len(key_parts), first, row_tile),
        out_shape=shapes,
        in_specs=[pl.BlockSpec(memory_space=pltpu.VMEM)] * (1 + len(key_parts) + len(state)),
        out_specs=tuple(pl.BlockSpec(memory_space=pltpu.VMEM) for _ in shapes),
        cost_estimate=pl.CostEstimate(
            flops=2 * rows * keys * (width + KVRANK),
            bytes_accessed=keys * width * 2 + rows * (width * 2 + KVRANK * 8),
            transcendentals=rows * keys,
        ),
        compiler_params=pltpu.CompilerParams(vmem_limit_bytes=24 * 1024 * 1024),
        name="attend",
    )(queries, *key_parts, *state)


def shifted(length, by):
    return [(i, (i + by) % length) for i in range(length)]


def along_z(chunk, chips):
    distance = chips // 2
    while distance:
        other = lax.ppermute(chunk, "z", shifted(chips, distance))
        chunk = jnp.concatenate([chunk, other], axis=0)
        distance //= 2
    return chunk


def on_device(
    chips,
    sides,
    query_latent,
    key_latent,
    rotary_key,
    query_gain,
    latent_gain,
    query_up,
    key_up,
    value_up,
    out_gain,
    out_weight,
):
    block_rows = query_latent.shape[0]
    row_count = key_latent.shape[0]
    head_local = key_up.shape[1] // NOPE_DIM
    block_start = (lax.axis_index("z") * CORES + lax.axis_index("core")) * block_rows
    own_start = block_start + lax.axis_index("tp") * row_count

    all_weight = lax.all_gather(out_weight, ("z", "core"), axis=0, tiled=True)

    latent_normed = rms_scaled(key_latent, latent_gain).astype(jnp.bfloat16)
    own_positions = (own_start + jnp.arange(row_count, dtype=jnp.int32)).astype(jnp.float32)
    key_turned = rotate_half(rotary_key, own_positions).astype(jnp.bfloat16)
    own = along_z(jnp.concatenate([latent_normed, key_turned], axis=1), chips)

    normed = rms_scaled(query_latent, query_gain).astype(jnp.bfloat16)
    query_full = jnp.dot(normed, query_up, preferred_element_type=jnp.float32).astype(jnp.bfloat16)
    query_full = query_full.reshape(block_rows, head_local, NOPE_DIM + ROPE_DIM)
    query_positions = (block_start + jnp.arange(block_rows, dtype=jnp.int32)).astype(jnp.float32)
    query_plain = query_full[..., :NOPE_DIM]
    query_turned = rotate_half(query_full[..., NOPE_DIM:], query_positions).astype(jnp.bfloat16)
    absorbed = jnp.einsum(
        "qhd,chd->hqc",
        query_plain,
        key_up.reshape(KVRANK, head_local, NOPE_DIM),
        preferred_element_type=jnp.float32,
    ).astype(jnp.bfloat16)
    queries = jnp.concatenate([absorbed, query_turned.transpose(1, 0, 2)], axis=-1)
    queries = queries.reshape(head_local * block_rows, KVRANK + ROPE_DIM)

    swap = [(i, (i + 1) % CORES) for i in range(CORES)]

    def partner(chunk):
        return lax.ppermute(chunk, "core", swap)

    right = lax.ppermute(own, "tp", shifted(sides, 1))
    left = lax.ppermute(own, "tp", shifted(sides, -1))
    half = own.shape[0] // 2
    far = [
        lax.ppermute(right[:half], "tp", shifted(sides, 1)),
        lax.ppermute(left[half:], "tp", shifted(sides, -1)),
    ]
    state = attend(queries, [own], None)
    state = attend(queries, [partner(own)], state)
    state = attend(queries, [right, left], state)
    state = attend(queries, [partner(right), partner(left)], state)
    state = attend(queries, far, state)
    state = attend(queries, [partner(f) for f in far], state)
    _, total, weighted = state

    latent_mix = (weighted / total[:, :1]).astype(jnp.bfloat16)
    latent_mix = latent_mix.reshape(head_local, block_rows, KVRANK)
    value_heads = value_up.reshape(KVRANK, head_local, VALUE_DIM)
    head_out = jnp.einsum(
        "hqc,chd->qhd", latent_mix, value_heads, preferred_element_type=jnp.float32
    ).astype(jnp.bfloat16)
    head_out = head_out.reshape(block_rows, head_local * VALUE_DIM)
    widened = head_out.astype(jnp.float32)
    square_part = jnp.sum(widened * widened, axis=1)
    gained = (widened * out_gain).astype(jnp.bfloat16)
    width = gained.shape[1]
    sent = jnp.concatenate(
        [
            gained,
            jnp.broadcast_to(square_part[:, None], (block_rows, 128)).astype(jnp.bfloat16),
        ],
        axis=1,
    )
    everyone = lax.all_gather(sent, "tp", axis=0)
    all_squares = jnp.sum(everyone[:, :, width].astype(jnp.float32), axis=0)
    own_sums = jnp.einsum(
        "xtk,xkn->tn",
        everyone[:, :, :width],
        all_weight.reshape(sides, width, all_weight.shape[1]),
        preferred_element_type=jnp.float32,
    )
    mean_square = all_squares / (HEADS * VALUE_DIM)
    return (own_sums * lax.rsqrt(mean_square + norm_eps)[:, None]).astype(jnp.bfloat16)


def solution(mesh):
    groups, places, sides = (mesh.shape[name] for name in ("grp", "sp", "tp"))
    chips = places // CORES
    fine = Mesh(
        mesh.devices.reshape(groups, chips, CORES, sides), ("grp", "z", "core", "tp")
    )
    tokens = ("grp", "z", "core")
    in_specs = (
        P(tokens, None),
        P((*tokens, "tp"), None),
        P((*tokens, "tp"), None),
        P(),
        P(),
        P(None, "tp"),
        P(None, "tp"),
        P(None, "tp"),
        P("tp"),
        P(("z", "core"), "tp"),
    )
    return jax.shard_map(
        functools.partial(on_device, chips, sides),
        mesh=fine,
        in_specs=in_specs,
        out_specs=P(tokens, "tp"),
        check_vma=False,
    )
```

```python
import functools

import jax
import jax.numpy as jnp
from jax import lax
from jax.experimental import pallas as pl
from jax.experimental.pallas import tpu as pltpu
from jax.sharding import Mesh
from jax.sharding import PartitionSpec as P

HEADS = 16
NOPE_DIM = 128
ROPE_DIM = 64
VALUE_DIM = 128
KVRANK = 256
CORES = 2


norm_eps = 1e-06
rope_theta = 10000.0
score_scale = (NOPE_DIM + ROPE_DIM) ** (-0.5)
exp2_scale = score_scale * 1.4426950408889634


def rms_scaled(inputs, gain_vec):
    widened = inputs.astype(jnp.float32)
    return (
        widened
        * lax.rsqrt(jnp.mean(widened * widened, axis=-1, keepdims=True) + norm_eps)
        * gain_vec
    )


def rotate_half(inputs, positions):
    half_width = inputs.shape[-1] // 2
    inverse = rope_theta ** (-jnp.arange(half_width, dtype=jnp.float32) / half_width)
    angles = positions[:, None] * inverse[None, :]
    if inputs.ndim == 3:
        angles = angles[:, None, :]
    cosine = jnp.cos(angles)
    sine = jnp.sin(angles)
    widened = inputs.astype(jnp.float32)
    first = widened[..., :half_width]
    second = widened[..., half_width:]
    return jnp.concatenate(
        [first * cosine - second * sine, second * cosine + first * sine], axis=-1
    )


def split_three(value):
    high = value.astype(jnp.bfloat16).astype(jnp.float32)
    rest = value - high
    middle = rest.astype(jnp.bfloat16).astype(jnp.float32)
    return high, middle, rest - middle


def as_row(column):
    return jnp.broadcast_to(column, (column.shape[0], 128)).T[:1, :]


def as_column(row):
    return jnp.broadcast_to(row, (128, row.shape[1])).T[:, :1]


def attend_kernel(n_keys, first, last, row_tile, q_ref, *refs):
    key_refs = refs[:n_keys]
    refs = refs[n_keys:]
    rows = q_ref.shape[0]
    if first:
        outs = refs
    else:
        stat_in, mix_in = refs[:2]
        outs = refs[2:]
    blocks = []
    for begin in range(0, rows, row_tile):
        span = pl.ds(begin, row_tile)
        q = q_ref[span, :]
        if first:
            top = total = mix = None
        else:
            top = stat_in[span, :1]
            total = stat_in[span, 64:65]
            mix = mix_in[span, :]
        for key_ref in key_refs:
            keys = key_ref[...]
            scores = lax.dot_general(
                q, keys, (((1,), (1,)), ((), ())), preferred_element_type=jnp.float32
            )
            here = jnp.max(scores, axis=1, keepdims=True)
            new_top = here if top is None else jnp.maximum(top, here)
            expo = jnp.exp2((scores - new_top) * exp2_scale)
            part = jnp.sum(expo, axis=1, keepdims=True)
            moved = jnp.dot(
                expo.astype(jnp.bfloat16),
                keys[:, :KVRANK],
                preferred_element_type=jnp.float32,
            )
            if top is None:
                total, mix = part, moved
            else:
                rescale = jnp.exp2((top - new_top) * exp2_scale)
                total = total * rescale + part
                mix = mix * rescale + moved
            top = new_top
        if last:
            outs[0][span, :] = (mix / total).astype(jnp.bfloat16)
            place = lax.broadcasted_iota(jnp.int32, (8, row_tile), 0)
            block = jnp.zeros((8, row_tile), jnp.float32)
            for k, row in enumerate((*split_three(as_row(top)), *split_three(as_row(total)))):
                block = jnp.where(place == k, row, block)
            blocks.append(block)
        else:
            lane = lax.broadcasted_iota(jnp.int32, (row_tile, 128), 1)
            outs[0][span, :] = jnp.where(lane < 64, top, total)
            outs[1][span, :] = mix
    if last:
        outs[0][pl.ds(rows, 8 * len(blocks)), :] = jnp.concatenate(blocks, axis=0).astype(
            jnp.bfloat16
        )


def attend(queries, key_parts, state=(), last=False, row_tile=256):
    rows, width = queries.shape
    keys = sum(k.shape[0] for k in key_parts)
    if last:
        shapes = (
            jax.ShapeDtypeStruct((rows + 8 * (rows // row_tile), KVRANK), jnp.bfloat16),
        )
    else:
        shapes = (
            jax.ShapeDtypeStruct((rows, 128), jnp.float32),
            jax.ShapeDtypeStruct((rows, KVRANK), jnp.float32),
        )
    return pl.pallas_call(
        functools.partial(attend_kernel, len(key_parts), not state, last, row_tile),
        out_shape=shapes,
        in_specs=[pl.BlockSpec(memory_space=pltpu.VMEM)] * (1 + len(key_parts) + len(state)),
        out_specs=tuple(pl.BlockSpec(memory_space=pltpu.VMEM) for _ in shapes),
        cost_estimate=pl.CostEstimate(
            flops=2 * rows * keys * (width + KVRANK),
            bytes_accessed=keys * width * 2 + rows * (width * 2 + KVRANK * 8),
            transcendentals=rows * keys,
        ),
        compiler_params=pltpu.CompilerParams(vmem_limit_bytes=16 * 1024 * 1024),
        name="attend",
    )(queries, *key_parts, *state)


def combine_kernel(row_tile, tokens, stat_ref, mix_ref, *refs):
    *part_refs, value_ref, gain_ref, out_ref = refs
    rows = mix_ref.shape[0]
    squares = jnp.zeros((tokens, 1), jnp.float32)
    for index, begin in enumerate(range(0, rows, row_tile)):
        span = pl.ds(begin, row_tile)
        tops = [stat_ref[span, :1]]
        sums = [stat_ref[span, 64:65]]
        for part_ref in part_refs:
            stats = part_ref[pl.ds(rows, 16), :].astype(jnp.float32)
            base = 8 * index
            top = stats[base : base + 1] + stats[base + 1 : base + 2] + stats[base + 2 : base + 3]
            total = (
                stats[base + 3 : base + 4] + stats[base + 4 : base + 5] + stats[base + 5 : base + 6]
            )
            tops.append(as_column(top))
            sums.append(as_column(total))
        best = functools.reduce(jnp.maximum, tops)
        rescale = jnp.exp2((tops[0] - best) * exp2_scale)
        whole = sums[0] * rescale
        mix = mix_ref[span, :] * rescale
        for part_ref, top, total in zip(part_refs, tops[1:], sums[1:]):
            weight = jnp.exp2((top - best) * exp2_scale) * total
            whole = whole + weight
            mix = mix + part_ref[span, :].astype(jnp.float32) * weight
        latent_mix = (mix / whole).astype(jnp.bfloat16)
        for offset in range(0, row_tile, tokens):
            head = (begin + offset) // tokens
            columns = pl.ds(head * VALUE_DIM, VALUE_DIM)
            head_out = jnp.dot(
                latent_mix[offset : offset + tokens],
                value_ref[:, columns],
                preferred_element_type=jnp.float32,
            ).astype(jnp.bfloat16)
            widened = head_out.astype(jnp.float32)
            squares = squares + jnp.sum(widened * widened, axis=1, keepdims=True)
            out_ref[:, columns] = (widened * gain_ref[:, columns]).astype(jnp.bfloat16)
    width = value_ref.shape[1]
    out_ref[:, pl.ds(width, 128)] = jnp.broadcast_to(squares, (tokens, 128)).astype(jnp.bfloat16)


def combine(state, parts, value_up, out_gain, tokens, row_tile=256):
    rows = state[1].shape[0]
    width = value_up.shape[1]
    return pl.pallas_call(
        functools.partial(combine_kernel, row_tile, tokens),
        out_shape=jax.ShapeDtypeStruct((tokens, width + 128), jnp.bfloat16),
        in_specs=[pl.BlockSpec(memory_space=pltpu.VMEM)] * (4 + len(parts)),
        out_specs=pl.BlockSpec(memory_space=pltpu.VMEM),
        cost_estimate=pl.CostEstimate(
            flops=2 * rows * KVRANK * VALUE_DIM,
            bytes_accessed=rows * KVRANK * 12,
            transcendentals=rows * 4,
        ),
        compiler_params=pltpu.CompilerParams(vmem_limit_bytes=16 * 1024 * 1024),
        name="combine",
    )(*state, *parts, value_up, out_gain[None, :])


def shifted(length, by):
    return [(i, (i + by) % length) for i in range(length)]


def on_device(
    chips,
    sides,
    query_latent,
    key_latent,
    rotary_key,
    query_gain,
    latent_gain,
    query_up,
    key_up,
    value_up,
    out_gain,
    out_weight,
):
    block_rows = query_latent.shape[0]
    row_count = key_latent.shape[0]
    head_local = key_up.shape[1] // NOPE_DIM
    block_start = (lax.axis_index("z") * CORES + lax.axis_index("core")) * block_rows
    own_start = block_start + lax.axis_index("tp") * row_count

    all_weight = lax.all_gather(out_weight, ("z", "core"), axis=0, tiled=True)

    latent_normed = rms_scaled(key_latent, latent_gain).astype(jnp.bfloat16)
    own_positions = (own_start + jnp.arange(row_count, dtype=jnp.int32)).astype(jnp.float32)
    key_turned = rotate_half(rotary_key, own_positions).astype(jnp.bfloat16)
    own = jnp.concatenate([latent_normed, key_turned], axis=1)
    across = lax.ppermute(own, "z", shifted(chips, chips // 2))
    half = row_count // 2
    up = jnp.concatenate([own[:half], across[:half]], axis=0)
    down = jnp.concatenate([own[half:], across[half:]], axis=0)

    normed = rms_scaled(query_latent, query_gain).astype(jnp.bfloat16)
    query_full = jnp.dot(normed, query_up, preferred_element_type=jnp.float32).astype(jnp.bfloat16)
    query_full = query_full.reshape(block_rows, head_local, NOPE_DIM + ROPE_DIM)
    query_positions = (block_start + jnp.arange(block_rows, dtype=jnp.int32)).astype(jnp.float32)
    query_plain = query_full[..., :NOPE_DIM]
    query_turned = rotate_half(query_full[..., NOPE_DIM:], query_positions).astype(jnp.bfloat16)
    absorbed = jnp.einsum(
        "qhd,chd->hqc",
        query_plain,
        key_up.reshape(KVRANK, head_local, NOPE_DIM),
        preferred_element_type=jnp.float32,
    ).astype(jnp.bfloat16)
    queries = jnp.concatenate([absorbed, query_turned.transpose(1, 0, 2)], axis=-1)
    queries = queries.reshape(head_local * block_rows, KVRANK + ROPE_DIM)

    distance = chips // 4
    up_next = lax.ppermute(up, "z", shifted(chips, distance))
    down_next = lax.ppermute(down, "z", shifted(chips, -distance))
    up_next, down_next, queries = lax.optimization_barrier((up_next, down_next, queries))
    turns = (2, 1, -1)
    guests = [lax.ppermute(queries, "tp", shifted(sides, by)) for by in turns]
    while True:
        up = jnp.concatenate([up, up_next], axis=0)
        down = jnp.concatenate([down, down_next], axis=0)
        distance //= 2
        if not distance:
            break
        up_next = lax.ppermute(up, "z", shifted(chips, distance))
        down_next = lax.ppermute(down, "z", shifted(chips, -distance))

    swap = [(i, (i + 1) % CORES) for i in range(CORES)]
    partner = [lax.ppermute(part, "core", swap) for part in (up, down)]
    states = [attend(guest, [up, down]) for guest in guests]
    state = attend(queries, [up, down])
    parts = []
    for by, guest, guest_state in zip(turns, guests, states):
        (part,) = attend(guest, partner, guest_state, last=True)
        parts.append(lax.ppermute(part, "tp", shifted(sides, -by)))
    state = attend(queries, partner, state)
    sent = combine(state, parts, value_up, out_gain, block_rows)
    width = value_up.shape[1]
    everyone = lax.all_gather(sent, "tp", axis=0)
    all_squares = jnp.sum(everyone[:, :, width].astype(jnp.float32), axis=0)
    own_sums = jnp.einsum(
        "xtk,xkn->tn",
        everyone[:, :, :width],
        all_weight.reshape(sides, width, all_weight.shape[1]),
        preferred_element_type=jnp.float32,
    )
    mean_square = all_squares / (HEADS * VALUE_DIM)
    return (own_sums * lax.rsqrt(mean_square + norm_eps)[:, None]).astype(jnp.bfloat16)


def solution(mesh):
    groups, places, sides = (mesh.shape[name] for name in ("grp", "sp", "tp"))
    chips = places // CORES
    fine = Mesh(
        mesh.devices.reshape(groups, chips, CORES, sides), ("grp", "z", "core", "tp")
    )
    tokens = ("grp", "z", "core")
    in_specs = (
        P(tokens, None),
        P((*tokens, "tp"), None),
        P((*tokens, "tp"), None),
        P(),
        P(),
        P(None, "tp"),
        P(None, "tp"),
        P(None, "tp"),
        P("tp"),
        P(("z", "core"), "tp"),
    )
    return jax.shard_map(
        functools.partial(on_device, chips, sides),
        mesh=fine,
        in_specs=in_specs,
        out_specs=P(tokens, "tp"),
        check_vma=False,
    )
```

```python
import functools

import jax
import jax.numpy as jnp
from jax import lax
from jax.experimental import pallas as pl
from jax.experimental.pallas import tpu as pltpu
from jax.sharding import Mesh
from jax.sharding import PartitionSpec as P


HEADS = 16
NOPE_DIM = 128
ROPE_DIM = 64
VALUE_DIM = 128
KVRANK = 256
CORES = 2


norm_eps = 1e-06
rope_theta = 10000.0
score_scale = (NOPE_DIM + ROPE_DIM) ** (-0.5)
exp2_scale = score_scale * 1.4426950408889634


def rms_scaled(inputs, gain_vec):
    widened = inputs.astype(jnp.float32)
    return (
        widened
        * lax.rsqrt(jnp.mean(widened * widened, axis=-1, keepdims=True) + norm_eps)
        * gain_vec
    )


def rotate_half(inputs, positions):
    half_width = inputs.shape[-1] // 2
    inverse = rope_theta ** (-jnp.arange(half_width, dtype=jnp.float32) / half_width)
    angles = positions[:, None] * inverse[None, :]
    if inputs.ndim == 3:
        angles = angles[:, None, :]
    cosine = jnp.cos(angles)
    sine = jnp.sin(angles)
    widened = inputs.astype(jnp.float32)
    first = widened[..., :half_width]
    second = widened[..., half_width:]
    return jnp.concatenate(
        [first * cosine - second * sine, second * cosine + first * sine], axis=-1
    )


def split_three(value):
    high = value.astype(jnp.bfloat16).astype(jnp.float32)
    rest = value - high
    middle = rest.astype(jnp.bfloat16).astype(jnp.float32)
    return high, middle, rest - middle


def as_row(column):
    return jnp.broadcast_to(column, (column.shape[0], 128)).T[:1, :]


def as_column(row):
    return jnp.broadcast_to(row, (128, row.shape[1])).T[:, :1]


def attend_kernel(guests, first, last, row_tile, *refs):
    query_refs, key_ref, refs = refs[:guests], refs[guests], refs[guests + 1 :]
    state_refs, outs = ((), refs) if first else (refs[: 2 * guests], refs[2 * guests :])
    rows = query_refs[0].shape[0]
    for guest in range(guests):
        blocks = []
        for begin in range(0, rows, row_tile):
            span = pl.ds(begin, row_tile)
            keys = key_ref[...]
            scores = lax.dot_general(
                query_refs[guest][span, :],
                keys,
                (((1,), (1,)), ((), ())),
                preferred_element_type=jnp.float32,
            )
            top = jnp.max(scores, axis=1, keepdims=True)
            if not first:
                stat_in, mix_in = state_refs[2 * guest : 2 * guest + 2]
                old_top = stat_in[span, :1]
                top = jnp.maximum(old_top, top)
            expo = jnp.exp2((scores - top) * exp2_scale)
            total = jnp.sum(expo, axis=1, keepdims=True)
            mix = jnp.dot(
                expo.astype(jnp.bfloat16),
                keys[:, :KVRANK],
                preferred_element_type=jnp.float32,
            )
            if not first:
                rescale = jnp.exp2((old_top - top) * exp2_scale)
                total = stat_in[span, 64:65] * rescale + total
                mix = mix_in[span, :] * rescale + mix
            if last:
                outs[0][span, :] = (mix / total).astype(jnp.bfloat16)
                place = lax.broadcasted_iota(jnp.int32, (8, row_tile), 0)
                block = jnp.zeros((8, row_tile), jnp.float32)
                for k, row in enumerate((*split_three(as_row(top)), *split_three(as_row(total)))):
                    block = jnp.where(place == k, row, block)
                blocks.append(block)
            else:
                lane = lax.broadcasted_iota(jnp.int32, (row_tile, 128), 1)
                outs[2 * guest][span, :] = jnp.where(lane < 64, top, total)
                outs[2 * guest + 1][span, :] = mix
        if last:
            outs[0][pl.ds(rows, 8 * len(blocks)), :] = jnp.concatenate(blocks, axis=0).astype(
                jnp.bfloat16
            )


def attend(queries, keys, state=(), last=False, row_tile=256):
    guests = len(queries)
    rows, width = queries[0].shape
    count = keys.shape[0]
    if last:
        shapes = (
            jax.ShapeDtypeStruct((rows + 8 * (rows // row_tile), KVRANK), jnp.bfloat16),
        )
    else:
        shapes = (
            jax.ShapeDtypeStruct((rows, 128), jnp.float32),
            jax.ShapeDtypeStruct((rows, KVRANK), jnp.float32),
        ) * guests
    return pl.pallas_call(
        functools.partial(attend_kernel, guests, not state, last, row_tile),
        out_shape=shapes,
        in_specs=[pl.BlockSpec(memory_space=pltpu.VMEM)] * (guests + 1 + len(state)),
        out_specs=tuple(pl.BlockSpec(memory_space=pltpu.VMEM) for _ in shapes),
        cost_estimate=pl.CostEstimate(
            flops=2 * guests * rows * count * (width + KVRANK),
            bytes_accessed=count * width * 2 + guests * rows * (width * 2 + KVRANK * 8),
            transcendentals=guests * rows * count,
        ),
        compiler_params=pltpu.CompilerParams(vmem_limit_bytes=20 * 1024 * 1024),
        name="attend",
    )(*queries, keys, *state)


def combine_kernel(row_tile, tokens, stat_ref, mix_ref, *refs):
    *part_refs, value_ref, gain_ref, out_ref = refs
    rows = mix_ref.shape[0]
    squares = jnp.zeros((tokens, 1), jnp.float32)
    for index, begin in enumerate(range(0, rows, row_tile)):
        span = pl.ds(begin, row_tile)
        tops = [stat_ref[span, :1]]
        sums = [stat_ref[span, 64:65]]
        for part_ref in part_refs:
            stats = part_ref[pl.ds(rows, 16), :].astype(jnp.float32)
            base = 8 * index
            top = stats[base : base + 1] + stats[base + 1 : base + 2] + stats[base + 2 : base + 3]
            total = (
                stats[base + 3 : base + 4] + stats[base + 4 : base + 5] + stats[base + 5 : base + 6]
            )
            tops.append(as_column(top))
            sums.append(as_column(total))
        best = functools.reduce(jnp.maximum, tops)
        rescale = jnp.exp2((tops[0] - best) * exp2_scale)
        whole = sums[0] * rescale
        mix = mix_ref[span, :] * rescale
        for part_ref, top, total in zip(part_refs, tops[1:], sums[1:]):
            weight = jnp.exp2((top - best) * exp2_scale) * total
            whole = whole + weight
            mix = mix + part_ref[span, :].astype(jnp.float32) * weight
        latent_mix = (mix / whole).astype(jnp.bfloat16)
        for offset in range(0, row_tile, tokens):
            head = (begin + offset) // tokens
            columns = pl.ds(head * VALUE_DIM, VALUE_DIM)
            head_out = jnp.dot(
                latent_mix[offset : offset + tokens],
                value_ref[:, columns],
                preferred_element_type=jnp.float32,
            ).astype(jnp.bfloat16)
            widened = head_out.astype(jnp.float32)
            squares = squares + jnp.sum(widened * widened, axis=1, keepdims=True)
            out_ref[:, columns] = (widened * gain_ref[:, columns]).astype(jnp.bfloat16)
    width = value_ref.shape[1]
    out_ref[:, pl.ds(width, 128)] = jnp.broadcast_to(squares, (tokens, 128)).astype(jnp.bfloat16)


def combine(state, parts, value_up, out_gain, tokens, row_tile=256):
    rows = state[1].shape[0]
    width = value_up.shape[1]
    return pl.pallas_call(
        functools.partial(combine_kernel, row_tile, tokens),
        out_shape=jax.ShapeDtypeStruct((tokens, width + 128), jnp.bfloat16),
        in_specs=[pl.BlockSpec(memory_space=pltpu.VMEM)] * (4 + len(parts)),
        out_specs=pl.BlockSpec(memory_space=pltpu.VMEM),
        cost_estimate=pl.CostEstimate(
            flops=2 * rows * KVRANK * VALUE_DIM,
            bytes_accessed=rows * KVRANK * 12,
            transcendentals=rows * 4,
        ),
        compiler_params=pltpu.CompilerParams(vmem_limit_bytes=16 * 1024 * 1024),
        name="combine",
    )(*state, *parts, value_up, out_gain[None, :])


def assemble_kernel(plan, n_in, *refs):
    sources, outs = refs[:n_in], refs[n_in:]
    for out, pieces in zip(outs, plan):
        at = 0
        for index, begin, count in pieces:
            out[pl.ds(at, count), :] = sources[index][pl.ds(begin, count), :]
            at += count


def assemble(sources, plan):
    shapes = tuple(
        jax.ShapeDtypeStruct((sum(p[2] for p in pieces), sources[0].shape[1]), sources[0].dtype)
        for pieces in plan
    )
    return pl.pallas_call(
        functools.partial(assemble_kernel, plan, len(sources)),
        out_shape=shapes,
        in_specs=[pl.BlockSpec(memory_space=pltpu.VMEM)] * len(sources),
        out_specs=tuple(pl.BlockSpec(memory_space=pltpu.VMEM) for _ in shapes),
        compiler_params=pltpu.CompilerParams(vmem_limit_bytes=8 * 1024 * 1024),
        name="assemble",
    )(*sources)


def prepare_kernel(
    latent_hbm, rotary_hbm, gain_hbm, cosine_ref, sine_ref, out_ref, latent_ref, rotary_ref, gain_ref, sems
):
    copies = [
        pltpu.make_async_copy(source, target, sems.at[k])
        for k, (source, target) in enumerate(
            ((latent_hbm, latent_ref), (rotary_hbm, rotary_ref), (gain_hbm, gain_ref))
        )
    ]
    for copy in copies:
        copy.start()
    for copy in copies:
        copy.wait()
    normed = rms_scaled(latent_ref[...], gain_ref[...])
    out_ref[:, :KVRANK] = normed.astype(jnp.bfloat16)
    widened = rotary_ref[...].astype(jnp.float32)
    half_width = ROPE_DIM // 2
    first, second = widened[:, :half_width], widened[:, half_width:]
    cosine, sine = cosine_ref[...], sine_ref[...]
    turned = jnp.concatenate(
        [first * cosine - second * sine, second * cosine + first * sine], axis=1
    )
    out_ref[:, KVRANK:] = turned.astype(jnp.bfloat16)


def prepare(key_latent, rotary_key, latent_gain, positions):
    rows = key_latent.shape[0]
    half_width = ROPE_DIM // 2
    inverse = rope_theta ** (-jnp.arange(half_width, dtype=jnp.float32) / half_width)
    angles = positions[:, None] * inverse[None, :]
    return pl.pallas_call(
        prepare_kernel,
        out_shape=jax.ShapeDtypeStruct((rows, KVRANK + ROPE_DIM), jnp.bfloat16),
        in_specs=[pl.BlockSpec(memory_space=pltpu.HBM)] * 3
        + [pl.BlockSpec(memory_space=pltpu.VMEM)] * 2,
        scratch_shapes=[
            pltpu.VMEM(key_latent.shape, key_latent.dtype),
            pltpu.VMEM(rotary_key.shape, rotary_key.dtype),
            pltpu.VMEM((1, latent_gain.shape[0]), latent_gain.dtype),
            pltpu.SemaphoreType.DMA((3,)),
        ],
        out_specs=pl.BlockSpec(memory_space=pltpu.VMEM),
        compiler_params=pltpu.CompilerParams(vmem_limit_bytes=8 * 1024 * 1024),
        name="prepare",
    )(key_latent, rotary_key, latent_gain[None, :], jnp.cos(angles), jnp.sin(angles))


def shifted(length, by):
    return [(i, (i + by) % length) for i in range(length)]


def on_device(
    chips,
    sides,
    query_latent,
    key_latent,
    rotary_key,
    query_gain,
    latent_gain,
    query_up,
    key_up,
    value_up,
    out_gain,
    out_weight,
):
    block_rows = query_latent.shape[0]
    row_count = key_latent.shape[0]
    head_local = key_up.shape[1] // NOPE_DIM
    block_start = (lax.axis_index("z") * CORES + lax.axis_index("core")) * block_rows
    own_start = block_start + lax.axis_index("tp") * row_count

    all_weight = lax.all_gather(out_weight, ("z", "core"), axis=0, tiled=True)

    own_positions = (own_start + jnp.arange(row_count, dtype=jnp.int32)).astype(jnp.float32)
    own = prepare(key_latent, rotary_key, latent_gain, own_positions)
    far = chips // 2
    others = []
    for by in (far, far // 2, -(far // 2)):
        others.append(lax.ppermute(own, "z", shifted(chips, by)))

    normed = rms_scaled(query_latent, query_gain).astype(jnp.bfloat16)
    query_full = jnp.dot(normed, query_up, preferred_element_type=jnp.float32)
    query_full = query_full.astype(jnp.bfloat16)
    query_full = query_full.reshape(block_rows, head_local, NOPE_DIM + ROPE_DIM)
    query_positions = (block_start + jnp.arange(block_rows, dtype=jnp.int32)).astype(jnp.float32)
    query_plain = query_full[..., :NOPE_DIM]
    query_turned = rotate_half(query_full[..., NOPE_DIM:], query_positions).astype(jnp.bfloat16)
    absorbed = jnp.einsum(
        "qhd,chd->hqc",
        query_plain,
        key_up.reshape(KVRANK, head_local, NOPE_DIM),
        preferred_element_type=jnp.float32,
    ).astype(jnp.bfloat16)
    queries = jnp.concatenate([absorbed, query_turned.transpose(1, 0, 2)], axis=-1)
    queries = queries.reshape(head_local * block_rows, KVRANK + ROPE_DIM)

    turns = (2, 1, -1)
    guests = []
    for by in turns:
        guests.append(lax.ppermute(queries, "tp", shifted(sides, by)))
    half = row_count // 2
    up, down = assemble(
        [own, *others], [[(k, begin, half) for k in range(4)] for begin in (0, half)]
    )
    distance = far // 4
    while distance > 1:
        up_next = lax.ppermute(up, "z", shifted(chips, distance))
        down_next = lax.ppermute(down, "z", shifted(chips, -distance))
        if distance == 2:
            up_next, down_next, *guests = lax.optimization_barrier((up_next, down_next, *guests))
        rows = up.shape[0]
        plan = [[(0, 0, rows), (1, 0, rows)], [(2, 0, rows), (3, 0, rows)]]
        if distance == 2:
            plan.append(plan[0] + plan[1])
        up, down, *near = assemble([up, up_next, down, down_next], plan)
        distance //= 2
    (near,) = near
    rows = up.shape[0]
    up_next = lax.ppermute(up, "z", shifted(chips, 1))
    down_next = lax.ppermute(down, "z", shifted(chips, -1))
    swap = [(i, (i + 1) % CORES) for i in range(CORES)]
    partner_near = lax.ppermute(near, "core", swap)
    everyone_asks = [*guests, queries]
    state = attend(everyone_asks, near)
    up_next, down_next, *state = lax.optimization_barrier((up_next, down_next, *state))
    (beside,) = assemble([up_next, down_next], [[(0, 0, rows), (1, 0, rows)]])
    partner_beside = lax.ppermute(beside, "core", swap)
    state = attend(everyone_asks, beside, state)
    state = attend(everyone_asks, partner_near, state)
    parts = []
    for k, by in enumerate(turns):
        (part,) = attend([guests[k]], partner_beside, state[2 * k : 2 * k + 2], last=True)
        parts.append(lax.ppermute(part, "tp", shifted(sides, -by)))
    state = attend([queries], partner_beside, state[2 * len(turns) :])
    sent = combine(state, parts, value_up, out_gain, block_rows)
    width = value_up.shape[1]
    everyone = lax.all_gather(sent, "tp", axis=0)
    all_squares = jnp.sum(everyone[:, :, width].astype(jnp.float32), axis=0)
    own_sums = jnp.einsum(
        "xtk,xkn->tn",
        everyone[:, :, :width],
        all_weight.reshape(sides, width, all_weight.shape[1]),
        preferred_element_type=jnp.float32,
    )
    mean_square = all_squares / (HEADS * VALUE_DIM)
    return (own_sums * lax.rsqrt(mean_square + norm_eps)[:, None]).astype(jnp.bfloat16)


def solution(mesh):
    groups, places, sides = (mesh.shape[name] for name in ("grp", "sp", "tp"))
    chips = places // CORES
    fine = Mesh(
        mesh.devices.reshape(groups, chips, CORES, sides), ("grp", "z", "core", "tp")
    )
    tokens = ("grp", "z", "core")
    in_specs = (
        P(tokens, None),
        P((*tokens, "tp"), None),
        P((*tokens, "tp"), None),
        P(),
        P(),
        P(None, "tp"),
        P(None, "tp"),
        P(None, "tp"),
        P("tp"),
        P(("z", "core"), "tp"),
    )
    return jax.shard_map(
        functools.partial(on_device, chips, sides),
        mesh=fine,
        in_specs=in_specs,
        out_specs=P(tokens, "tp"),
        check_vma=False,
    )
```

```python
import functools

import jax
import jax.numpy as jnp
from jax import lax
from jax.experimental import pallas as pl
from jax.experimental.pallas import tpu as pltpu
from jax.sharding import Mesh
from jax.sharding import PartitionSpec as P


HEADS = 16
NOPE_DIM = 128
ROPE_DIM = 64
VALUE_DIM = 128
KVRANK = 256
CORES = 2


norm_eps = 1e-06
rope_theta = 10000.0
score_scale = (NOPE_DIM + ROPE_DIM) ** (-0.5)
exp2_scale = score_scale * 1.4426950408889634


def rms_scaled(inputs, gain_vec):
    widened = inputs.astype(jnp.float32)
    return (
        widened
        * lax.rsqrt(jnp.mean(widened * widened, axis=-1, keepdims=True) + norm_eps)
        * gain_vec
    )


def rotate_half(inputs, positions):
    half_width = inputs.shape[-1] // 2
    inverse = rope_theta ** (-jnp.arange(half_width, dtype=jnp.float32) / half_width)
    angles = positions[:, None] * inverse[None, :]
    if inputs.ndim == 3:
        angles = angles[:, None, :]
    cosine = jnp.cos(angles)
    sine = jnp.sin(angles)
    widened = inputs.astype(jnp.float32)
    first = widened[..., :half_width]
    second = widened[..., half_width:]
    return jnp.concatenate(
        [first * cosine - second * sine, second * cosine + first * sine], axis=-1
    )


def split_three(value):
    high = value.astype(jnp.bfloat16).astype(jnp.float32)
    rest = value - high
    middle = rest.astype(jnp.bfloat16).astype(jnp.float32)
    return high, middle, rest - middle


def as_column(row):
    return jnp.broadcast_to(row, (128, row.shape[1])).T[:, :1]


def attend_kernel(guests, first, last, chunk, *refs):
    query_refs, key_ref, refs = refs[:guests], refs[guests], refs[guests + 1 :]
    state_refs, outs = ((), refs) if first else (refs[: 2 * guests], refs[2 * guests :])
    rows = query_refs[0].shape[0]
    for guest in range(guests):
        stat_ref, mix_ref = outs[-2:] if last else outs[2 * guest : 2 * guest + 2]
        keys = key_ref[...]
        scores = lax.dot_general(
            query_refs[guest][...],
            keys,
            (((1,), (1,)), ((), ())),
            preferred_element_type=jnp.float32,
        )
        top = jnp.max(scores, axis=1, keepdims=True)
        expo = jnp.exp2((scores - top) * exp2_scale)
        total = jnp.sum(expo, axis=1, keepdims=True)
        mix_ref[...] = jnp.dot(
            expo.astype(jnp.bfloat16), keys[:, :KVRANK], preferred_element_type=jnp.float32
        )
        lane = lax.broadcasted_iota(jnp.int32, (rows, 128), 1)
        stat_ref[...] = jnp.where(lane < 64, top, total)
        if first:
            continue
        stat_in, mix_in = state_refs[2 * guest : 2 * guest + 2]
        for begin in range(0, rows, chunk):
            span = pl.ds(begin, chunk)
            new, old = stat_ref[span, :], stat_in[span, :]
            best = jnp.maximum(new[:, :1], old[:, :1])
            new_scale = jnp.exp2((new[:, :1] - best) * exp2_scale)
            old_scale = jnp.exp2((old[:, :1] - best) * exp2_scale)
            mix = mix_ref[span, :] * new_scale + mix_in[span, :] * old_scale
            totals = new * new_scale + old * old_scale
            lane = lax.broadcasted_iota(jnp.int32, (chunk, 128), 1)
            stat_ref[span, :] = jnp.where(lane < 64, best, totals)
            if last:
                outs[0][span, :] = (mix / totals[:, 64:65]).astype(jnp.bfloat16)
            else:
                mix_ref[span, :] = mix
    if last:
        width = mix_ref.shape[1]
        blocks = []
        for begin in range(0, rows, width):
            turned = stat_ref[pl.ds(begin, width), :].T
            place = lax.broadcasted_iota(jnp.int32, (8, width), 0)
            block = jnp.zeros((8, width), jnp.float32)
            for k, row in enumerate((*split_three(turned[:1]), *split_three(turned[64:65]))):
                block = jnp.where(place == k, row, block)
            blocks.append(block)
        outs[0][pl.ds(rows, 8 * len(blocks)), :] = jnp.concatenate(blocks, axis=0).astype(
            jnp.bfloat16
        )


def attend(queries, keys, state=(), last=False):
    guests = len(queries)
    rows, width = queries[0].shape
    count = keys.shape[0]
    scratch = []
    if last:
        shapes = (jax.ShapeDtypeStruct((rows + 8 * (rows // KVRANK), KVRANK), jnp.bfloat16),)
        scratch = [pltpu.VMEM((rows, 128), jnp.float32), pltpu.VMEM((rows, KVRANK), jnp.float32)]
    else:
        shapes = (
            jax.ShapeDtypeStruct((rows, 128), jnp.float32),
            jax.ShapeDtypeStruct((rows, KVRANK), jnp.float32),
        ) * guests
    return pl.pallas_call(
        functools.partial(attend_kernel, guests, not state, last, 64),
        out_shape=shapes,
        in_specs=[pl.BlockSpec(memory_space=pltpu.VMEM)] * (guests + 1 + len(state)),
        out_specs=tuple(pl.BlockSpec(memory_space=pltpu.VMEM) for _ in shapes),
        scratch_shapes=scratch,
        cost_estimate=pl.CostEstimate(
            flops=2 * guests * rows * count * (width + KVRANK),
            bytes_accessed=count * width * 2 + guests * rows * (width * 2 + KVRANK * 8),
            transcendentals=guests * rows * count,
        ),
        compiler_params=pltpu.CompilerParams(vmem_limit_bytes=20 * 1024 * 1024),
        name="attend",
    )(*queries, keys, *state)


def combine_kernel(row_tile, tokens, stat_ref, mix_ref, *refs):
    *part_refs, value_ref, gain_ref, out_ref = refs
    rows = mix_ref.shape[0]
    squares = jnp.zeros((tokens, 1), jnp.float32)
    for index, begin in enumerate(range(0, rows, row_tile)):
        span = pl.ds(begin, row_tile)
        tops = [stat_ref[span, :1]]
        sums = [stat_ref[span, 64:65]]
        for part_ref in part_refs:
            stats = part_ref[pl.ds(rows, 16), :].astype(jnp.float32)
            base = 8 * index
            top = stats[base : base + 1] + stats[base + 1 : base + 2] + stats[base + 2 : base + 3]
            total = (
                stats[base + 3 : base + 4] + stats[base + 4 : base + 5] + stats[base + 5 : base + 6]
            )
            tops.append(as_column(top))
            sums.append(as_column(total))
        best = functools.reduce(jnp.maximum, tops)
        rescale = jnp.exp2((tops[0] - best) * exp2_scale)
        whole = sums[0] * rescale
        mix = mix_ref[span, :] * rescale
        for part_ref, top, total in zip(part_refs, tops[1:], sums[1:]):
            weight = jnp.exp2((top - best) * exp2_scale) * total
            whole = whole + weight
            mix = mix + part_ref[span, :].astype(jnp.float32) * weight
        latent_mix = (mix / whole).astype(jnp.bfloat16)
        for offset in range(0, row_tile, tokens):
            head = (begin + offset) // tokens
            columns = pl.ds(head * VALUE_DIM, VALUE_DIM)
            head_out = jnp.dot(
                latent_mix[offset : offset + tokens],
                value_ref[:, columns],
                preferred_element_type=jnp.float32,
            ).astype(jnp.bfloat16)
            widened = head_out.astype(jnp.float32)
            squares = squares + jnp.sum(widened * widened, axis=1, keepdims=True)
            out_ref[:, columns] = (widened * gain_ref[:, columns]).astype(jnp.bfloat16)
    width = value_ref.shape[1]
    out_ref[:, pl.ds(width, 128)] = jnp.broadcast_to(squares, (tokens, 128)).astype(jnp.bfloat16)


def combine(state, parts, value_up, out_gain, tokens, row_tile=256):
    rows = state[1].shape[0]
    width = value_up.shape[1]
    return pl.pallas_call(
        functools.partial(combine_kernel, row_tile, tokens),
        out_shape=jax.ShapeDtypeStruct((tokens, width + 128), jnp.bfloat16),
        in_specs=[pl.BlockSpec(memory_space=pltpu.VMEM)] * (4 + len(parts)),
        out_specs=pl.BlockSpec(memory_space=pltpu.VMEM),
        cost_estimate=pl.CostEstimate(
            flops=2 * rows * KVRANK * VALUE_DIM,
            bytes_accessed=rows * KVRANK * 12,
            transcendentals=rows * 4,
        ),
        compiler_params=pltpu.CompilerParams(vmem_limit_bytes=16 * 1024 * 1024),
        name="combine",
    )(*state, *parts, value_up, out_gain[None, :])


def assemble_kernel(plan, n_in, *refs):
    sources, outs = refs[:n_in], refs[n_in:]
    for out, pieces in zip(outs, plan):
        at = 0
        for index, begin, count in pieces:
            out[pl.ds(at, count), :] = sources[index][pl.ds(begin, count), :]
            at += count


def assemble(sources, plan):
    shapes = tuple(
        jax.ShapeDtypeStruct((sum(p[2] for p in pieces), sources[0].shape[1]), sources[0].dtype)
        for pieces in plan
    )
    return pl.pallas_call(
        functools.partial(assemble_kernel, plan, len(sources)),
        out_shape=shapes,
        in_specs=[pl.BlockSpec(memory_space=pltpu.VMEM)] * len(sources),
        out_specs=tuple(pl.BlockSpec(memory_space=pltpu.VMEM) for _ in shapes),
        compiler_params=pltpu.CompilerParams(vmem_limit_bytes=8 * 1024 * 1024),
        name="assemble",
    )(*sources)


def prepare_kernel(
    latent_hbm, rotary_hbm, gain_hbm, cosine_ref, sine_ref, out_ref, latent_ref, rotary_ref, gain_ref, sems
):
    copies = [
        pltpu.make_async_copy(source, target, sems.at[k])
        for k, (source, target) in enumerate(
            ((latent_hbm, latent_ref), (rotary_hbm, rotary_ref), (gain_hbm, gain_ref))
        )
    ]
    for copy in copies:
        copy.start()
    for copy in copies:
        copy.wait()
    normed = rms_scaled(latent_ref[...], gain_ref[...])
    out_ref[:, :KVRANK] = normed.astype(jnp.bfloat16)
    widened = rotary_ref[...].astype(jnp.float32)
    half_width = ROPE_DIM // 2
    first, second = widened[:, :half_width], widened[:, half_width:]
    cosine, sine = cosine_ref[...], sine_ref[...]
    turned = jnp.concatenate(
        [first * cosine - second * sine, second * cosine + first * sine], axis=1
    )
    out_ref[:, KVRANK:] = turned.astype(jnp.bfloat16)


def prepare(key_latent, rotary_key, latent_gain, positions):
    rows = key_latent.shape[0]
    half_width = ROPE_DIM // 2
    inverse = rope_theta ** (-jnp.arange(half_width, dtype=jnp.float32) / half_width)
    angles = positions[:, None] * inverse[None, :]
    return pl.pallas_call(
        prepare_kernel,
        out_shape=jax.ShapeDtypeStruct((rows, KVRANK + ROPE_DIM), jnp.bfloat16),
        in_specs=[pl.BlockSpec(memory_space=pltpu.HBM)] * 3
        + [pl.BlockSpec(memory_space=pltpu.VMEM)] * 2,
        scratch_shapes=[
            pltpu.VMEM(key_latent.shape, key_latent.dtype),
            pltpu.VMEM(rotary_key.shape, rotary_key.dtype),
            pltpu.VMEM((1, latent_gain.shape[0]), latent_gain.dtype),
            pltpu.SemaphoreType.DMA((3,)),
        ],
        out_specs=pl.BlockSpec(memory_space=pltpu.VMEM),
        compiler_params=pltpu.CompilerParams(vmem_limit_bytes=8 * 1024 * 1024),
        name="prepare",
    )(key_latent, rotary_key, latent_gain[None, :], jnp.cos(angles), jnp.sin(angles))


def shifted(length, by):
    return [(i, (i + by) % length) for i in range(length)]


def on_device(
    chips,
    sides,
    query_latent,
    key_latent,
    rotary_key,
    query_gain,
    latent_gain,
    query_up,
    key_up,
    value_up,
    out_gain,
    out_weight,
):
    block_rows = query_latent.shape[0]
    row_count = key_latent.shape[0]
    head_local = key_up.shape[1] // NOPE_DIM
    block_start = (lax.axis_index("z") * CORES + lax.axis_index("core")) * block_rows
    own_start = block_start + lax.axis_index("tp") * row_count

    all_weight = lax.all_gather(out_weight, ("z", "core"), axis=0, tiled=True)

    own_positions = (own_start + jnp.arange(row_count, dtype=jnp.int32)).astype(jnp.float32)
    own = prepare(key_latent, rotary_key, latent_gain, own_positions)
    far = chips // 2
    others = []
    for by in (far, far // 2, -(far // 2)):
        others.append(lax.ppermute(own, "z", shifted(chips, by)))

    normed = rms_scaled(query_latent, query_gain).astype(jnp.bfloat16)
    query_full = jnp.dot(normed, query_up, preferred_element_type=jnp.float32)
    query_full = query_full.astype(jnp.bfloat16)
    query_full = query_full.reshape(block_rows, head_local, NOPE_DIM + ROPE_DIM)
    query_positions = (block_start + jnp.arange(block_rows, dtype=jnp.int32)).astype(jnp.float32)
    query_plain = query_full[..., :NOPE_DIM]
    query_turned = rotate_half(query_full[..., NOPE_DIM:], query_positions).astype(jnp.bfloat16)
    absorbed = jnp.einsum(
        "qhd,chd->hqc",
        query_plain,
        key_up.reshape(KVRANK, head_local, NOPE_DIM),
        preferred_element_type=jnp.float32,
    ).astype(jnp.bfloat16)
    queries = jnp.concatenate([absorbed, query_turned.transpose(1, 0, 2)], axis=-1)
    queries = queries.reshape(head_local * block_rows, KVRANK + ROPE_DIM)

    turns = (2, 1, -1)
    guests = []
    for by in turns:
        guests.append(lax.ppermute(queries, "tp", shifted(sides, by)))
    half = row_count // 2
    up, down = assemble(
        [own, *others], [[(k, begin, half) for k in range(4)] for begin in (0, half)]
    )
    distance = far // 4
    while distance > 1:
        up_next = lax.ppermute(up, "z", shifted(chips, distance))
        down_next = lax.ppermute(down, "z", shifted(chips, -distance))
        if distance == 2:
            up_next, down_next, *guests = lax.optimization_barrier((up_next, down_next, *guests))
        rows = up.shape[0]
        plan = [[(0, 0, rows), (1, 0, rows)], [(2, 0, rows), (3, 0, rows)]]
        if distance == 2:
            plan.append(plan[0] + plan[1])
        up, down, *near = assemble([up, up_next, down, down_next], plan)
        distance //= 2
    (near,) = near
    rows = up.shape[0]
    up_next = lax.ppermute(up, "z", shifted(chips, 1))
    down_next = lax.ppermute(down, "z", shifted(chips, -1))
    swap = [(i, (i + 1) % CORES) for i in range(CORES)]
    partner_near = lax.ppermute(near, "core", swap)
    everyone_asks = [*guests, queries]
    state = attend(everyone_asks, near)
    up_next, down_next, *state = lax.optimization_barrier((up_next, down_next, *state))
    (beside,) = assemble([up_next, down_next], [[(0, 0, rows), (1, 0, rows)]])
    partner_beside = lax.ppermute(beside, "core", swap)
    state = attend(everyone_asks, beside, state)
    state = attend(everyone_asks, partner_near, state)
    parts = []
    for k, by in enumerate(turns):
        (part,) = attend([guests[k]], partner_beside, state[2 * k : 2 * k + 2], last=True)
        parts.append(lax.ppermute(part, "tp", shifted(sides, -by)))
    state = attend([queries], partner_beside, state[2 * len(turns) :])
    sent = combine(state, parts, value_up, out_gain, block_rows)
    width = value_up.shape[1]
    everyone = lax.all_gather(sent, "tp", axis=0)
    all_squares = jnp.sum(everyone[:, :, width].astype(jnp.float32), axis=0)
    own_sums = jnp.einsum(
        "xtk,xkn->tn",
        everyone[:, :, :width],
        all_weight.reshape(sides, width, all_weight.shape[1]),
        preferred_element_type=jnp.float32,
    )
    mean_square = all_squares / (HEADS * VALUE_DIM)
    return (own_sums * lax.rsqrt(mean_square + norm_eps)[:, None]).astype(jnp.bfloat16)


def solution(mesh):
    groups, places, sides = (mesh.shape[name] for name in ("grp", "sp", "tp"))
    chips = places // CORES
    fine = Mesh(
        mesh.devices.reshape(groups, chips, CORES, sides), ("grp", "z", "core", "tp")
    )
    tokens = ("grp", "z", "core")
    in_specs = (
        P(tokens, None),
        P((*tokens, "tp"), None),
        P((*tokens, "tp"), None),
        P(),
        P(),
        P(None, "tp"),
        P(None, "tp"),
        P(None, "tp"),
        P("tp"),
        P(("z", "core"), "tp"),
    )
    return jax.shard_map(
        functools.partial(on_device, chips, sides),
        mesh=fine,
        in_specs=in_specs,
        out_specs=P(tokens, "tp"),
        check_vma=False,
    )
```

```python
import functools

import jax
import jax.numpy as jnp
from jax import lax
from jax.experimental import pallas as pl
from jax.experimental.pallas import tpu as pltpu
from jax.sharding import Mesh
from jax.sharding import PartitionSpec as P


HEADS = 16
NOPE_DIM = 128
ROPE_DIM = 64
VALUE_DIM = 128
KVRANK = 256
CORES = 2


norm_eps = 1e-06
rope_theta = 10000.0
score_scale = (NOPE_DIM + ROPE_DIM) ** (-0.5)
exp2_scale = score_scale * 1.4426950408889634


def rms_scaled(inputs, gain_vec):
    widened = inputs.astype(jnp.float32)
    return (
        widened
        * lax.rsqrt(jnp.mean(widened * widened, axis=-1, keepdims=True) + norm_eps)
        * gain_vec
    )


def rotate_half(inputs, positions):
    half_width = inputs.shape[-1] // 2
    inverse = rope_theta ** (-jnp.arange(half_width, dtype=jnp.float32) / half_width)
    angles = positions[:, None] * inverse[None, :]
    if inputs.ndim == 3:
        angles = angles[:, None, :]
    cosine = jnp.cos(angles)
    sine = jnp.sin(angles)
    widened = inputs.astype(jnp.float32)
    first = widened[..., :half_width]
    second = widened[..., half_width:]
    return jnp.concatenate(
        [first * cosine - second * sine, second * cosine + first * sine], axis=-1
    )


def split_three(value):
    high = value.astype(jnp.bfloat16).astype(jnp.float32)
    rest = value - high
    middle = rest.astype(jnp.bfloat16).astype(jnp.float32)
    return high, middle, rest - middle


def as_column(row):
    return jnp.broadcast_to(row, (128, row.shape[1])).T[:, :1]


def attend_kernel(guests, first, last, chunk, *refs):
    query_refs, key_ref, refs = refs[:guests], refs[guests], refs[guests + 1 :]
    state_refs, outs = ((), refs) if first else (refs[: 2 * guests], refs[2 * guests :])
    rows = query_refs[0].shape[0]
    for guest in range(guests):
        stat_ref, mix_ref = outs[-2:] if last else outs[2 * guest : 2 * guest + 2]
        keys = key_ref[...]
        scores = lax.dot_general(
            query_refs[guest][...],
            keys,
            (((1,), (1,)), ((), ())),
            preferred_element_type=jnp.float32,
        )
        top = jnp.max(scores, axis=1, keepdims=True)
        expo = jnp.exp2((scores - top) * exp2_scale)
        total = jnp.sum(expo, axis=1, keepdims=True)
        mix_ref[...] = jnp.dot(
            expo.astype(jnp.bfloat16), keys[:, :KVRANK], preferred_element_type=jnp.float32
        )
        lane = lax.broadcasted_iota(jnp.int32, (rows, 128), 1)
        stat_ref[...] = jnp.where(lane < 64, top, total)
        if first:
            continue
        stat_in, mix_in = state_refs[2 * guest : 2 * guest + 2]
        for begin in range(0, rows, chunk):
            span = pl.ds(begin, chunk)
            new, old = stat_ref[span, :], stat_in[span, :]
            best = jnp.maximum(new[:, :1], old[:, :1])
            new_scale = jnp.exp2((new[:, :1] - best) * exp2_scale)
            old_scale = jnp.exp2((old[:, :1] - best) * exp2_scale)
            mix = mix_ref[span, :] * new_scale + mix_in[span, :] * old_scale
            totals = new * new_scale + old * old_scale
            lane = lax.broadcasted_iota(jnp.int32, (chunk, 128), 1)
            stat_ref[span, :] = jnp.where(lane < 64, best, totals)
            if last:
                outs[0][span, :] = (mix / totals[:, 64:65]).astype(jnp.bfloat16)
            else:
                mix_ref[span, :] = mix
    if last:
        width = mix_ref.shape[1]
        blocks = []
        for begin in range(0, rows, width):
            turned = stat_ref[pl.ds(begin, width), :].T
            place = lax.broadcasted_iota(jnp.int32, (8, width), 0)
            block = jnp.zeros((8, width), jnp.float32)
            for k, row in enumerate((*split_three(turned[:1]), *split_three(turned[64:65]))):
                block = jnp.where(place == k, row, block)
            blocks.append(block)
        outs[0][pl.ds(rows, 8 * len(blocks)), :] = jnp.concatenate(blocks, axis=0).astype(
            jnp.bfloat16
        )


def attend(queries, keys, state=(), last=False):
    guests = len(queries)
    rows, width = queries[0].shape
    count = keys.shape[0]
    scratch = []
    if last:
        shapes = (jax.ShapeDtypeStruct((rows + 8 * (rows // KVRANK), KVRANK), jnp.bfloat16),)
        scratch = [pltpu.VMEM((rows, 128), jnp.float32), pltpu.VMEM((rows, KVRANK), jnp.float32)]
    else:
        shapes = (
            jax.ShapeDtypeStruct((rows, 128), jnp.float32),
            jax.ShapeDtypeStruct((rows, KVRANK), jnp.float32),
        ) * guests
    return pl.pallas_call(
        functools.partial(attend_kernel, guests, not state, last, 64),
        out_shape=shapes,
        in_specs=[pl.BlockSpec(memory_space=pltpu.VMEM)] * (guests + 1 + len(state)),
        out_specs=tuple(pl.BlockSpec(memory_space=pltpu.VMEM) for _ in shapes),
        scratch_shapes=scratch,
        cost_estimate=pl.CostEstimate(
            flops=2 * guests * rows * count * (width + KVRANK),
            bytes_accessed=count * width * 2 + guests * rows * (width * 2 + KVRANK * 8),
            transcendentals=guests * rows * count,
        ),
        compiler_params=pltpu.CompilerParams(vmem_limit_bytes=20 * 1024 * 1024),
        name="attend",
    )(*queries, keys, *state)


def combine_kernel(row_tile, tokens, stat_ref, mix_ref, *refs):
    *part_refs, value_ref, gain_ref, out_ref = refs
    rows = mix_ref.shape[0]
    squares = jnp.zeros((tokens, 1), jnp.float32)
    for index, begin in enumerate(range(0, rows, row_tile)):
        span = pl.ds(begin, row_tile)
        tops = [stat_ref[span, :1]]
        sums = [stat_ref[span, 64:65]]
        for part_ref in part_refs:
            stats = part_ref[pl.ds(rows, 16), :].astype(jnp.float32)
            base = 8 * index
            top = stats[base : base + 1] + stats[base + 1 : base + 2] + stats[base + 2 : base + 3]
            total = (
                stats[base + 3 : base + 4] + stats[base + 4 : base + 5] + stats[base + 5 : base + 6]
            )
            tops.append(as_column(top))
            sums.append(as_column(total))
        best = functools.reduce(jnp.maximum, tops)
        rescale = jnp.exp2((tops[0] - best) * exp2_scale)
        whole = sums[0] * rescale
        mix = mix_ref[span, :] * rescale
        for part_ref, top, total in zip(part_refs, tops[1:], sums[1:]):
            weight = jnp.exp2((top - best) * exp2_scale) * total
            whole = whole + weight
            mix = mix + part_ref[span, :].astype(jnp.float32) * weight
        latent_mix = (mix / whole).astype(jnp.bfloat16)
        for offset in range(0, row_tile, tokens):
            head = (begin + offset) // tokens
            columns = pl.ds(head * VALUE_DIM, VALUE_DIM)
            head_out = jnp.dot(
                latent_mix[offset : offset + tokens],
                value_ref[:, columns],
                preferred_element_type=jnp.float32,
            ).astype(jnp.bfloat16)
            widened = head_out.astype(jnp.float32)
            squares = squares + jnp.sum(widened * widened, axis=1, keepdims=True)
            out_ref[:, columns] = (widened * gain_ref[:, columns]).astype(jnp.bfloat16)
    width = value_ref.shape[1]
    out_ref[:, pl.ds(width, 128)] = jnp.broadcast_to(squares, (tokens, 128)).astype(jnp.bfloat16)


def combine(state, parts, value_up, out_gain, tokens, row_tile=256):
    rows = state[1].shape[0]
    width = value_up.shape[1]
    return pl.pallas_call(
        functools.partial(combine_kernel, row_tile, tokens),
        out_shape=jax.ShapeDtypeStruct((tokens, width + 128), jnp.bfloat16),
        in_specs=[pl.BlockSpec(memory_space=pltpu.VMEM)] * (4 + len(parts)),
        out_specs=pl.BlockSpec(memory_space=pltpu.VMEM),
        cost_estimate=pl.CostEstimate(
            flops=2 * rows * KVRANK * VALUE_DIM,
            bytes_accessed=rows * KVRANK * 12,
            transcendentals=rows * 4,
        ),
        compiler_params=pltpu.CompilerParams(vmem_limit_bytes=16 * 1024 * 1024),
        name="combine",
    )(*state, *parts, value_up, out_gain[None, :])


def assemble_kernel(plan, n_in, *refs):
    sources, outs = refs[:n_in], refs[n_in:]
    for out, pieces in zip(outs, plan):
        at = 0
        for index, begin, count in pieces:
            out[pl.ds(at, count), :] = sources[index][pl.ds(begin, count), :]
            at += count


def assemble(sources, plan):
    shapes = tuple(
        jax.ShapeDtypeStruct((sum(p[2] for p in pieces), sources[0].shape[1]), sources[0].dtype)
        for pieces in plan
    )
    return pl.pallas_call(
        functools.partial(assemble_kernel, plan, len(sources)),
        out_shape=shapes,
        in_specs=[pl.BlockSpec(memory_space=pltpu.VMEM)] * len(sources),
        out_specs=tuple(pl.BlockSpec(memory_space=pltpu.VMEM) for _ in shapes),
        compiler_params=pltpu.CompilerParams(vmem_limit_bytes=8 * 1024 * 1024),
        name="assemble",
    )(*sources)


def prepare_kernel(
    latent_hbm, rotary_hbm, gain_hbm, cosine_ref, sine_ref, out_ref, latent_ref, rotary_ref, gain_ref, sems
):
    copies = [
        pltpu.make_async_copy(source, target, sems.at[k])
        for k, (source, target) in enumerate(
            ((latent_hbm, latent_ref), (rotary_hbm, rotary_ref), (gain_hbm, gain_ref))
        )
    ]
    for copy in copies:
        copy.start()
    for copy in copies:
        copy.wait()
    normed = rms_scaled(latent_ref[...], gain_ref[...])
    out_ref[:, :KVRANK] = normed.astype(jnp.bfloat16)
    widened = rotary_ref[...].astype(jnp.float32)
    half_width = ROPE_DIM // 2
    first, second = widened[:, :half_width], widened[:, half_width:]
    cosine, sine = cosine_ref[...], sine_ref[...]
    turned = jnp.concatenate(
        [first * cosine - second * sine, second * cosine + first * sine], axis=1
    )
    out_ref[:, KVRANK:] = turned.astype(jnp.bfloat16)


def prepare(key_latent, rotary_key, latent_gain, positions):
    rows = key_latent.shape[0]
    half_width = ROPE_DIM // 2
    inverse = rope_theta ** (-jnp.arange(half_width, dtype=jnp.float32) / half_width)
    angles = positions[:, None] * inverse[None, :]
    return pl.pallas_call(
        prepare_kernel,
        out_shape=jax.ShapeDtypeStruct((rows, KVRANK + ROPE_DIM), jnp.bfloat16),
        in_specs=[pl.BlockSpec(memory_space=pltpu.HBM)] * 3
        + [pl.BlockSpec(memory_space=pltpu.VMEM)] * 2,
        scratch_shapes=[
            pltpu.VMEM(key_latent.shape, key_latent.dtype),
            pltpu.VMEM(rotary_key.shape, rotary_key.dtype),
            pltpu.VMEM((1, latent_gain.shape[0]), latent_gain.dtype),
            pltpu.SemaphoreType.DMA((3,)),
        ],
        out_specs=pl.BlockSpec(memory_space=pltpu.VMEM),
        compiler_params=pltpu.CompilerParams(vmem_limit_bytes=8 * 1024 * 1024),
        name="prepare",
    )(key_latent, rotary_key, latent_gain[None, :], jnp.cos(angles), jnp.sin(angles))


def project_kernel(
    blocks, everyone_hbm, weight_hbm, out_ref, everyone_ref, weight_ref, total, sems
):
    depth = weight_ref.shape[0] // blocks
    sides, _, width = everyone_ref.shape
    width -= 128
    shared = width // depth
    activations = pltpu.make_async_copy(everyone_hbm, everyone_ref, sems.at[blocks])
    activations.start()
    copies = []
    for block in range(blocks):
        span = pl.ds(block * depth, depth)
        copies.append(
            pltpu.make_async_copy(weight_hbm.at[span, :], weight_ref.at[span, :], sems.at[block])
        )
        copies[-1].start()
    activations.wait()
    squares = sum(
        everyone_ref[side, :, pl.ds(width, 128)].astype(jnp.float32) for side in range(sides)
    )
    scale = lax.rsqrt(squares[:, :1] / (HEADS * VALUE_DIM) + norm_eps)
    for block in range(blocks):
        copies[block].wait()
        product = jnp.dot(
            everyone_ref[block // shared, :, pl.ds(block % shared * depth, depth)],
            weight_ref[pl.ds(block * depth, depth), :],
            preferred_element_type=jnp.float32,
        )
        if block == 0:
            total[...] = product
        elif block < blocks - 1:
            total[...] += product
        else:
            out_ref[...] = ((total[...] + product) * scale).astype(jnp.bfloat16)


def project(everyone, weight, blocks=8):
    tokens = everyone.shape[1]
    depth, features = weight.shape
    return pl.pallas_call(
        functools.partial(project_kernel, blocks),
        out_shape=jax.ShapeDtypeStruct((tokens, features), jnp.bfloat16),
        in_specs=[pl.BlockSpec(memory_space=pltpu.HBM)] * 2,
        out_specs=pl.BlockSpec(memory_space=pltpu.VMEM),
        scratch_shapes=[
            pltpu.VMEM(everyone.shape, everyone.dtype),
            pltpu.VMEM(weight.shape, weight.dtype),
            pltpu.VMEM((tokens, features), jnp.float32),
            pltpu.SemaphoreType.DMA((blocks + 1,)),
        ],
        cost_estimate=pl.CostEstimate(
            flops=2 * tokens * depth * features,
            bytes_accessed=depth * features * 2,
            transcendentals=0,
        ),
        compiler_params=pltpu.CompilerParams(vmem_limit_bytes=60 * 1024 * 1024),
        name="project",
    )(everyone, weight)


def shifted(length, by):
    return [(i, (i + by) % length) for i in range(length)]


def on_device(
    chips,
    sides,
    query_latent,
    key_latent,
    rotary_key,
    query_gain,
    latent_gain,
    query_up,
    key_up,
    value_up,
    out_gain,
    out_weight,
):
    block_rows = query_latent.shape[0]
    row_count = key_latent.shape[0]
    head_local = key_up.shape[1] // NOPE_DIM
    block_start = (lax.axis_index("z") * CORES + lax.axis_index("core")) * block_rows
    own_start = block_start + lax.axis_index("tp") * row_count

    all_weight = lax.all_gather(out_weight, ("z", "core"), axis=0, tiled=True)

    own_positions = (own_start + jnp.arange(row_count, dtype=jnp.int32)).astype(jnp.float32)
    own = prepare(key_latent, rotary_key, latent_gain, own_positions)
    far = chips // 2
    others = []
    for by in (far, far // 2, -(far // 2)):
        others.append(lax.ppermute(own, "z", shifted(chips, by)))

    normed = rms_scaled(query_latent, query_gain).astype(jnp.bfloat16)
    query_full = jnp.dot(normed, query_up, preferred_element_type=jnp.float32)
    query_full = query_full.astype(jnp.bfloat16)
    query_full = query_full.reshape(block_rows, head_local, NOPE_DIM + ROPE_DIM)
    query_positions = (block_start + jnp.arange(block_rows, dtype=jnp.int32)).astype(jnp.float32)
    query_plain = query_full[..., :NOPE_DIM]
    query_turned = rotate_half(query_full[..., NOPE_DIM:], query_positions).astype(jnp.bfloat16)
    absorbed = jnp.einsum(
        "qhd,chd->hqc",
        query_plain,
        key_up.reshape(KVRANK, head_local, NOPE_DIM),
        preferred_element_type=jnp.float32,
    ).astype(jnp.bfloat16)
    queries = jnp.concatenate([absorbed, query_turned.transpose(1, 0, 2)], axis=-1)
    queries = queries.reshape(head_local * block_rows, KVRANK + ROPE_DIM)

    turns = (2, 1, -1)
    guests = []
    for by in turns:
        guests.append(lax.ppermute(queries, "tp", shifted(sides, by)))
    half = row_count // 2
    up, down = assemble(
        [own, *others], [[(k, begin, half) for k in range(4)] for begin in (0, half)]
    )
    distance = far // 4
    while distance > 1:
        up_next = lax.ppermute(up, "z", shifted(chips, distance))
        down_next = lax.ppermute(down, "z", shifted(chips, -distance))
        rows = up.shape[0]
        plan = [[(0, 0, rows), (1, 0, rows)], [(2, 0, rows), (3, 0, rows)]]
        if distance == 2:
            plan.append(plan[0] + plan[1])
        up, down, *near = assemble([up, up_next, down, down_next], plan)
        distance //= 2
    (near,) = near
    rows = up.shape[0]
    up_next = lax.ppermute(up, "z", shifted(chips, 1))
    down_next = lax.ppermute(down, "z", shifted(chips, -1))
    swap = [(i, (i + 1) % CORES) for i in range(CORES)]
    partner_near = lax.ppermute(near, "core", swap)
    everyone_asks = [*guests, queries]
    state = attend(everyone_asks, near)
    up_next, down_next, *state = lax.optimization_barrier((up_next, down_next, *state))
    (beside,) = assemble([up_next, down_next], [[(0, 0, rows), (1, 0, rows)]])
    partner_beside = lax.ppermute(beside, "core", swap)
    state = attend(everyone_asks, beside, state)
    state = attend(everyone_asks, partner_near, state)
    parts = []
    for k, by in enumerate(turns):
        (part,) = attend([guests[k]], partner_beside, state[2 * k : 2 * k + 2], last=True)
        parts.append(lax.ppermute(part, "tp", shifted(sides, -by)))
    state = attend([queries], partner_beside, state[2 * len(turns) :])
    sent = combine(state, parts, value_up, out_gain, block_rows)
    everyone = lax.all_gather(sent, "tp", axis=0)
    return project(everyone, all_weight)


def solution(mesh):
    groups, places, sides = (mesh.shape[name] for name in ("grp", "sp", "tp"))
    chips = places // CORES
    fine = Mesh(
        mesh.devices.reshape(groups, chips, CORES, sides), ("grp", "z", "core", "tp")
    )
    tokens = ("grp", "z", "core")
    in_specs = (
        P(tokens, None),
        P((*tokens, "tp"), None),
        P((*tokens, "tp"), None),
        P(),
        P(),
        P(None, "tp"),
        P(None, "tp"),
        P(None, "tp"),
        P("tp"),
        P(("z", "core"), "tp"),
    )
    return jax.shard_map(
        functools.partial(on_device, chips, sides),
        mesh=fine,
        in_specs=in_specs,
        out_specs=P(tokens, "tp"),
        check_vma=False,
    )
```

```python
import functools

import jax
import jax.numpy as jnp
from jax import lax
from jax.experimental import pallas as pl
from jax.experimental.pallas import tpu as pltpu
from jax.sharding import Mesh
from jax.sharding import PartitionSpec as P


HEADS = 16
NOPE_DIM = 128
ROPE_DIM = 64
VALUE_DIM = 128
KVRANK = 256
CORES = 2


norm_eps = 1e-06
rope_theta = 10000.0
score_scale = (NOPE_DIM + ROPE_DIM) ** (-0.5)
exp2_scale = score_scale * 1.4426950408889634


def rms_scaled(inputs, gain_vec):
    widened = inputs.astype(jnp.float32)
    return (
        widened
        * lax.rsqrt(jnp.mean(widened * widened, axis=-1, keepdims=True) + norm_eps)
        * gain_vec
    )


def rotate_half(inputs, positions):
    half_width = inputs.shape[-1] // 2
    inverse = rope_theta ** (-jnp.arange(half_width, dtype=jnp.float32) / half_width)
    angles = positions[:, None] * inverse[None, :]
    if inputs.ndim == 3:
        angles = angles[:, None, :]
    cosine = jnp.cos(angles)
    sine = jnp.sin(angles)
    widened = inputs.astype(jnp.float32)
    first = widened[..., :half_width]
    second = widened[..., half_width:]
    return jnp.concatenate(
        [first * cosine - second * sine, second * cosine + first * sine], axis=-1
    )


def split_three(value):
    high = value.astype(jnp.bfloat16).astype(jnp.float32)
    rest = value - high
    middle = rest.astype(jnp.bfloat16).astype(jnp.float32)
    return high, middle, rest - middle


def as_column(row):
    return jnp.broadcast_to(row, (128, row.shape[1])).T[:, :1]


def attend_kernel(guests, first, last, chunk, *refs):
    query_refs, key_ref, refs = refs[:guests], refs[guests], refs[guests + 1 :]
    state_refs, outs = ((), refs) if first else (refs[: 2 * guests], refs[2 * guests :])
    rows = query_refs[0].shape[0]
    for guest in range(guests):
        stat_ref, mix_ref = outs[-2:] if last else outs[2 * guest : 2 * guest + 2]
        keys = key_ref[...]
        scores = lax.dot_general(
            query_refs[guest][...],
            keys,
            (((1,), (1,)), ((), ())),
            preferred_element_type=jnp.float32,
        )
        top = jnp.max(scores, axis=1, keepdims=True)
        expo = jnp.exp2((scores - top) * exp2_scale)
        total = jnp.sum(expo, axis=1, keepdims=True)
        mix_ref[...] = jnp.dot(
            expo.astype(jnp.bfloat16), keys[:, :KVRANK], preferred_element_type=jnp.float32
        )
        lane = lax.broadcasted_iota(jnp.int32, (rows, 128), 1)
        stat_ref[...] = jnp.where(lane < 64, top, total)
        if first:
            continue
        stat_in, mix_in = state_refs[2 * guest : 2 * guest + 2]
        for begin in range(0, rows, chunk):
            span = pl.ds(begin, chunk)
            new, old = stat_ref[span, :], stat_in[span, :]
            best = jnp.maximum(new[:, :1], old[:, :1])
            new_scale = jnp.exp2((new[:, :1] - best) * exp2_scale)
            old_scale = jnp.exp2((old[:, :1] - best) * exp2_scale)
            mix = mix_ref[span, :] * new_scale + mix_in[span, :] * old_scale
            totals = new * new_scale + old * old_scale
            lane = lax.broadcasted_iota(jnp.int32, (chunk, 128), 1)
            stat_ref[span, :] = jnp.where(lane < 64, best, totals)
            if last:
                outs[0][span, :] = (mix / totals[:, 64:65]).astype(jnp.bfloat16)
            else:
                mix_ref[span, :] = mix
    if last:
        width = mix_ref.shape[1]
        blocks = []
        for begin in range(0, rows, width):
            turned = stat_ref[pl.ds(begin, width), :].T
            place = lax.broadcasted_iota(jnp.int32, (8, width), 0)
            block = jnp.zeros((8, width), jnp.float32)
            for k, row in enumerate((*split_three(turned[:1]), *split_three(turned[64:65]))):
                block = jnp.where(place == k, row, block)
            blocks.append(block)
        outs[0][pl.ds(rows, 8 * len(blocks)), :] = jnp.concatenate(blocks, axis=0).astype(
            jnp.bfloat16
        )


def attend(queries, keys, state=(), last=False):
    guests = len(queries)
    rows, width = queries[0].shape
    count = keys.shape[0]
    scratch = []
    if last:
        shapes = (jax.ShapeDtypeStruct((rows + 8 * (rows // KVRANK), KVRANK), jnp.bfloat16),)
        scratch = [pltpu.VMEM((rows, 128), jnp.float32), pltpu.VMEM((rows, KVRANK), jnp.float32)]
    else:
        shapes = (
            jax.ShapeDtypeStruct((rows, 128), jnp.float32),
            jax.ShapeDtypeStruct((rows, KVRANK), jnp.float32),
        ) * guests
    return pl.pallas_call(
        functools.partial(attend_kernel, guests, not state, last, 64),
        out_shape=shapes,
        in_specs=[pl.BlockSpec(memory_space=pltpu.VMEM)] * (guests + 1 + len(state)),
        out_specs=tuple(pl.BlockSpec(memory_space=pltpu.VMEM) for _ in shapes),
        scratch_shapes=scratch,
        cost_estimate=pl.CostEstimate(
            flops=2 * guests * rows * count * (width + KVRANK),
            bytes_accessed=count * width * 2 + guests * rows * (width * 2 + KVRANK * 8),
            transcendentals=guests * rows * count,
        ),
        compiler_params=pltpu.CompilerParams(vmem_limit_bytes=20 * 1024 * 1024),
        name="attend",
    )(*queries, keys, *state)


def combine_kernel(row_tile, tokens, stat_ref, mix_ref, *refs):
    *part_refs, value_ref, gain_ref, out_ref = refs
    rows = mix_ref.shape[0]
    squares = jnp.zeros((tokens, 1), jnp.float32)
    for index, begin in enumerate(range(0, rows, row_tile)):
        span = pl.ds(begin, row_tile)
        tops = [stat_ref[span, :1]]
        sums = [stat_ref[span, 64:65]]
        for part_ref in part_refs:
            stats = part_ref[pl.ds(rows, 16), :].astype(jnp.float32)
            base = 8 * index
            top = stats[base : base + 1] + stats[base + 1 : base + 2] + stats[base + 2 : base + 3]
            total = (
                stats[base + 3 : base + 4] + stats[base + 4 : base + 5] + stats[base + 5 : base + 6]
            )
            tops.append(as_column(top))
            sums.append(as_column(total))
        best = functools.reduce(jnp.maximum, tops)
        rescale = jnp.exp2((tops[0] - best) * exp2_scale)
        whole = sums[0] * rescale
        mix = mix_ref[span, :] * rescale
        for part_ref, top, total in zip(part_refs, tops[1:], sums[1:]):
            weight = jnp.exp2((top - best) * exp2_scale) * total
            whole = whole + weight
            mix = mix + part_ref[span, :].astype(jnp.float32) * weight
        latent_mix = (mix / whole).astype(jnp.bfloat16)
        for offset in range(0, row_tile, tokens):
            head = (begin + offset) // tokens
            columns = pl.ds(head * VALUE_DIM, VALUE_DIM)
            head_out = jnp.dot(
                latent_mix[offset : offset + tokens],
                value_ref[:, columns],
                preferred_element_type=jnp.float32,
            ).astype(jnp.bfloat16)
            widened = head_out.astype(jnp.float32)
            squares = squares + jnp.sum(widened * widened, axis=1, keepdims=True)
            out_ref[:, columns] = (widened * gain_ref[:, columns]).astype(jnp.bfloat16)
    width = value_ref.shape[1]
    out_ref[:, pl.ds(width, 128)] = jnp.broadcast_to(squares, (tokens, 128)).astype(jnp.bfloat16)


def combine(state, parts, value_up, out_gain, tokens, row_tile=256):
    rows = state[1].shape[0]
    width = value_up.shape[1]
    return pl.pallas_call(
        functools.partial(combine_kernel, row_tile, tokens),
        out_shape=jax.ShapeDtypeStruct((tokens, width + 128), jnp.bfloat16),
        in_specs=[pl.BlockSpec(memory_space=pltpu.VMEM)] * (4 + len(parts)),
        out_specs=pl.BlockSpec(memory_space=pltpu.VMEM),
        cost_estimate=pl.CostEstimate(
            flops=2 * rows * KVRANK * VALUE_DIM,
            bytes_accessed=rows * KVRANK * 12,
            transcendentals=rows * 4,
        ),
        compiler_params=pltpu.CompilerParams(vmem_limit_bytes=16 * 1024 * 1024),
        name="combine",
    )(*state, *parts, value_up, out_gain[None, :])


def assemble_kernel(plan, n_in, *refs):
    sources, outs = refs[:n_in], refs[n_in:]
    for out, pieces in zip(outs, plan):
        at = 0
        for index, begin, count in pieces:
            out[pl.ds(at, count), :] = sources[index][pl.ds(begin, count), :]
            at += count


def assemble(sources, plan):
    shapes = tuple(
        jax.ShapeDtypeStruct((sum(p[2] for p in pieces), sources[0].shape[1]), sources[0].dtype)
        for pieces in plan
    )
    return pl.pallas_call(
        functools.partial(assemble_kernel, plan, len(sources)),
        out_shape=shapes,
        in_specs=[pl.BlockSpec(memory_space=pltpu.VMEM)] * len(sources),
        out_specs=tuple(pl.BlockSpec(memory_space=pltpu.VMEM) for _ in shapes),
        compiler_params=pltpu.CompilerParams(vmem_limit_bytes=8 * 1024 * 1024),
        name="assemble",
    )(*sources)


def prepare_kernel(
    latent_hbm, rotary_hbm, gain_hbm, cosine_ref, sine_ref, out_ref, latent_ref, rotary_ref, gain_ref, sems
):
    copies = [
        pltpu.make_async_copy(source, target, sems.at[k])
        for k, (source, target) in enumerate(
            ((latent_hbm, latent_ref), (rotary_hbm, rotary_ref), (gain_hbm, gain_ref))
        )
    ]
    for copy in copies:
        copy.start()
    for copy in copies:
        copy.wait()
    normed = rms_scaled(latent_ref[...], gain_ref[...])
    out_ref[:, :KVRANK] = normed.astype(jnp.bfloat16)
    widened = rotary_ref[...].astype(jnp.float32)
    half_width = ROPE_DIM // 2
    first, second = widened[:, :half_width], widened[:, half_width:]
    cosine, sine = cosine_ref[...], sine_ref[...]
    turned = jnp.concatenate(
        [first * cosine - second * sine, second * cosine + first * sine], axis=1
    )
    out_ref[:, KVRANK:] = turned.astype(jnp.bfloat16)


def prepare(key_latent, rotary_key, latent_gain, positions):
    rows = key_latent.shape[0]
    half_width = ROPE_DIM // 2
    inverse = rope_theta ** (-jnp.arange(half_width, dtype=jnp.float32) / half_width)
    angles = positions[:, None] * inverse[None, :]
    return pl.pallas_call(
        prepare_kernel,
        out_shape=jax.ShapeDtypeStruct((rows, KVRANK + ROPE_DIM), jnp.bfloat16),
        in_specs=[pl.BlockSpec(memory_space=pltpu.HBM)] * 3
        + [pl.BlockSpec(memory_space=pltpu.VMEM)] * 2,
        scratch_shapes=[
            pltpu.VMEM(key_latent.shape, key_latent.dtype),
            pltpu.VMEM(rotary_key.shape, rotary_key.dtype),
            pltpu.VMEM((1, latent_gain.shape[0]), latent_gain.dtype),
            pltpu.SemaphoreType.DMA((3,)),
        ],
        out_specs=pl.BlockSpec(memory_space=pltpu.VMEM),
        compiler_params=pltpu.CompilerParams(vmem_limit_bytes=8 * 1024 * 1024),
        name="prepare",
    )(key_latent, rotary_key, latent_gain[None, :], jnp.cos(angles), jnp.sin(angles))


def project_kernel(
    blocks, halves, everyone_hbm, weight_hbm, out_ref, everyone_ref, weight_ref, total, sems
):
    step = pl.program_id(0)
    depth = weight_ref.shape[1] // blocks
    part = weight_ref.shape[2]
    sides, _, width = everyone_ref.shape
    width -= 128
    shared = width // depth
    activations = pltpu.make_async_copy(everyone_hbm, everyone_ref, sems.at[halves, 0])

    def weights(half, block):
        span = pl.ds(block * depth, depth)
        return pltpu.make_async_copy(
            weight_hbm.at[span, pl.ds(half * part, part)],
            weight_ref.at[half, span, :],
            sems.at[half, block],
        )

    @pl.when(step == 0)
    def _():
        activations.start()
        for half in range(halves):
            for block in range(blocks):
                weights(half, block).start()
        activations.wait()

    squares = sum(
        everyone_ref[side, :, pl.ds(width, 128)].astype(jnp.float32) for side in range(sides)
    )
    scale = lax.rsqrt(squares[:, :1] / (HEADS * VALUE_DIM) + norm_eps)
    for half in range(halves):

        @pl.when(step == half)
        def _():
            for block in range(blocks):
                weights(half, block).wait()
                product = jnp.dot(
                    everyone_ref[block // shared, :, pl.ds(block % shared * depth, depth)],
                    weight_ref[half, pl.ds(block * depth, depth), :],
                    preferred_element_type=jnp.float32,
                )
                if block == 0:
                    total[...] = product
                elif block < blocks - 1:
                    total[...] += product
                else:
                    out_ref[...] = ((total[...] + product) * scale).astype(jnp.bfloat16)


def project(everyone, weight, blocks=4, halves=2):
    tokens = everyone.shape[1]
    depth, features = weight.shape
    part = features // halves
    return pl.pallas_call(
        functools.partial(project_kernel, blocks, halves),
        grid=(halves,),
        out_shape=jax.ShapeDtypeStruct((tokens, features), jnp.bfloat16),
        in_specs=[pl.BlockSpec(memory_space=pltpu.HBM)] * 2,
        out_specs=pl.BlockSpec((tokens, part), lambda step: (0, step)),
        scratch_shapes=[
            pltpu.VMEM(everyone.shape, everyone.dtype),
            pltpu.VMEM((halves, depth, part), weight.dtype),
            pltpu.VMEM((tokens, part), jnp.float32),
            pltpu.SemaphoreType.DMA((halves + 1, blocks)),
        ],
        cost_estimate=pl.CostEstimate(
            flops=2 * tokens * depth * features,
            bytes_accessed=depth * features * 2,
            transcendentals=0,
        ),
        compiler_params=pltpu.CompilerParams(vmem_limit_bytes=60 * 1024 * 1024),
        name="project",
    )(everyone, weight)


def shifted(length, by):
    return [(i, (i + by) % length) for i in range(length)]


def on_device(
    chips,
    sides,
    query_latent,
    key_latent,
    rotary_key,
    query_gain,
    latent_gain,
    query_up,
    key_up,
    value_up,
    out_gain,
    out_weight,
):
    block_rows = query_latent.shape[0]
    row_count = key_latent.shape[0]
    head_local = key_up.shape[1] // NOPE_DIM
    block_start = (lax.axis_index("z") * CORES + lax.axis_index("core")) * block_rows
    own_start = block_start + lax.axis_index("tp") * row_count

    all_weight = lax.all_gather(out_weight, ("z", "core"), axis=0, tiled=True)

    own_positions = (own_start + jnp.arange(row_count, dtype=jnp.int32)).astype(jnp.float32)
    own = prepare(key_latent, rotary_key, latent_gain, own_positions)
    far = chips // 2
    others = []
    for by in (far, far // 2, -(far // 2)):
        others.append(lax.ppermute(own, "z", shifted(chips, by)))

    normed = rms_scaled(query_latent, query_gain).astype(jnp.bfloat16)
    query_full = jnp.dot(normed, query_up, preferred_element_type=jnp.float32)
    query_full = query_full.astype(jnp.bfloat16)
    query_full = query_full.reshape(block_rows, head_local, NOPE_DIM + ROPE_DIM)
    query_positions = (block_start + jnp.arange(block_rows, dtype=jnp.int32)).astype(jnp.float32)
    query_plain = query_full[..., :NOPE_DIM]
    query_turned = rotate_half(query_full[..., NOPE_DIM:], query_positions).astype(jnp.bfloat16)
    absorbed = jnp.einsum(
        "qhd,chd->hqc",
        query_plain,
        key_up.reshape(KVRANK, head_local, NOPE_DIM),
        preferred_element_type=jnp.float32,
    ).astype(jnp.bfloat16)
    queries = jnp.concatenate([absorbed, query_turned.transpose(1, 0, 2)], axis=-1)
    queries = queries.reshape(head_local * block_rows, KVRANK + ROPE_DIM)

    turns = (2, 1, -1)
    guests = []
    for by in turns:
        guests.append(lax.ppermute(queries, "tp", shifted(sides, by)))
    half = row_count // 2
    up, down = assemble(
        [own, *others], [[(k, begin, half) for k in range(4)] for begin in (0, half)]
    )
    distance = far // 4
    while distance > 1:
        up_next = lax.ppermute(up, "z", shifted(chips, distance))
        down_next = lax.ppermute(down, "z", shifted(chips, -distance))
        rows = up.shape[0]
        plan = [[(0, 0, rows), (1, 0, rows)], [(2, 0, rows), (3, 0, rows)]]
        if distance == 2:
            plan.append(plan[0] + plan[1])
        up, down, *near = assemble([up, up_next, down, down_next], plan)
        distance //= 2
    (near,) = near
    rows = up.shape[0]
    up_next = lax.ppermute(up, "z", shifted(chips, 1))
    down_next = lax.ppermute(down, "z", shifted(chips, -1))
    swap = [(i, (i + 1) % CORES) for i in range(CORES)]
    partner_near = lax.ppermute(near, "core", swap)
    everyone_asks = [*guests, queries]
    state = attend(everyone_asks, near)
    up_next, down_next, *state = lax.optimization_barrier((up_next, down_next, *state))
    (beside,) = assemble([up_next, down_next], [[(0, 0, rows), (1, 0, rows)]])
    partner_beside = lax.ppermute(beside, "core", swap)
    state = attend(everyone_asks, beside, state)
    state = attend(everyone_asks, partner_near, state)
    parts = []
    for k, by in enumerate(turns):
        (part,) = attend([guests[k]], partner_beside, state[2 * k : 2 * k + 2], last=True)
        parts.append(lax.ppermute(part, "tp", shifted(sides, -by)))
    state = attend([queries], partner_beside, state[2 * len(turns) :])
    sent = combine(state, parts, value_up, out_gain, block_rows)
    everyone = lax.all_gather(sent, "tp", axis=0)
    return project(everyone, all_weight)


def solution(mesh):
    groups, places, sides = (mesh.shape[name] for name in ("grp", "sp", "tp"))
    chips = places // CORES
    fine = Mesh(
        mesh.devices.reshape(groups, chips, CORES, sides), ("grp", "z", "core", "tp")
    )
    tokens = ("grp", "z", "core")
    in_specs = (
        P(tokens, None),
        P((*tokens, "tp"), None),
        P((*tokens, "tp"), None),
        P(),
        P(),
        P(None, "tp"),
        P(None, "tp"),
        P(None, "tp"),
        P("tp"),
        P(("z", "core"), "tp"),
    )
    return jax.shard_map(
        functools.partial(on_device, chips, sides),
        mesh=fine,
        in_specs=in_specs,
        out_specs=P(tokens, "tp"),
        check_vma=False,
    )
```
